128 devices in a mesh: sp: 16 (over z, x), tp: 8 (over y, core).
Axes of the slice: x: 4, y: 4, z: 4, core: 2. Of those that a mesh axis runs over, the one named last changes fastest.
Arguments:
- block_input: bfloat16 [32768, 4096], P('sp'), may hold values from -6 to 6
- value_weight: bfloat16 [4096, 1024], P(None, 'tp'), may hold values from -0.09375 to 0.09375
- key_rows: bfloat16 [32768, 512], P('sp', 'tp'), may hold values from -1 to 1
- query_rows: bfloat16 [32768, 512], P('sp', 'tp'), may hold values from -1 to 1
- decay_pre: float32 [16, 32768], P('tp', 'sp'), may hold values from -3 to 2
- decay_log: float32 [16], P('tp'), may hold values from -16 to -2
- gate_rows: bfloat16 [32768, 1024], P('sp', 'tp'), may hold values from -6 to 6
- out_grad: bfloat16 [32768, 1024], P('sp', 'tp'), may hold values from -6 to 6
Outputs:
- key_grad: float32 [32768, 512], P('sp', 'tp')
- query_grad: float32 [32768, 512], P('sp', 'tp')
- decay_grad: float32 [16, 32768], P('tp', 'sp')
- gate_grad: float32 [32768, 1024], P('sp', 'tp')
- weight_grad: float32 [4096, 1024], P('sp', 'tp')
- row_norms: float32 [4096], P('sp')
The draws below stay inside these ranges and needn't reach their ends.
All inputs are finite; a program needn't handle non-finite values.
Results may differ from the reference program's by a relative error of at most 0.0035.
Values sent between devices are 32-bit elements; how exact they have to be, the bound alone decides.
A program may use at most 128 MiB of HBM per device.

```python
import jax
import jax.numpy as jnp
from jax import lax

D = 4096
HEADS = 16
HEAD = 64
GROUPS = 8
STATE = 64
BLK = 128
TOK_DEV = 2048
TOKENS = 32768


def draw_decay_log(key, part):
    pick_key, slow_key, fast_key = jax.random.split(jax.random.fold_in(key, 11), 3)
    slow_share = 0.5
    is_slow = jax.random.uniform(pick_key, (HEADS,), jnp.float32) < slow_share
    slow_rate = jax.random.uniform(slow_key, (HEADS,), jnp.float32, 0.25, 0.5) / TOKENS
    fast_rate = jax.random.uniform(fast_key, (HEADS,), jnp.float32, 0.05, 0.1)
    return jnp.log(jnp.where(is_slow, slow_rate, fast_rate)).astype(jnp.float32)


def draw_decay_pre(key, part):
    level_key, noise_key = jax.random.split(jax.random.fold_in(key, 23), 2)
    levels = jax.random.uniform(level_key, (HEADS, TOKENS // TOK_DEV), jnp.float32, -1.5, 1.0)
    noise = jax.random.uniform(noise_key, (HEADS, TOKENS), jnp.float32, -0.99, 0.99)
    return (jnp.repeat(levels, TOK_DEV, axis=1) + noise).astype(jnp.float32)


def raised(array, key, source, target, blocks, factor):
    def block_of(position):
        return (jnp.arange(array.shape[position]) // (array.shape[position] // blocks)).reshape((-1,) + (1,) * (array.ndim - 1 - position))

    one_side = jax.random.permutation(key, blocks)[block_of(target)]
    other_side = (block_of(target) + blocks // 2) % blocks
    return jnp.where((block_of(source) == one_side) | (block_of(source) == other_side), factor * array, array)


def steps_of(stream_key, shape, cuts, least, high):
    factor_of, own = 1.0, jax.random.fold_in(stream_key, 6)
    for dim, shards_of in cuts:
        heights = jnp.exp(jax.random.uniform(jax.random.fold_in(own, dim), (shards_of,), jnp.float32, least / len(cuts), high / len(cuts)))
        factor_of = factor_of * jnp.repeat(heights, shape[dim] // shards_of).reshape([-1 if axis == dim else 1 for axis in range(len(shape))])
    return factor_of


def bell_draw(key, shape, width, most, cuts=(), dtype=jnp.bfloat16):
    level = steps_of(key, shape, cuts, -0.22, 0.18) if cuts else 1.0
    drawn = jax.random.normal(key, shape, jnp.float32) * width * level
    return jnp.minimum(jnp.maximum(drawn, -most), most).astype(dtype)


def noise_with(own_key, dims, scale, most, cuts, heavy, kind=jnp.bfloat16):
    entries = scale * jax.random.normal(own_key, dims, jnp.float32)
    if cuts:
        entries = entries * steps_of(own_key, dims, cuts, -0.22, 0.18)
    return jnp.clip(raised(entries, jax.random.fold_in(own_key, 3), *heavy), -most, most).astype(kind)


def setup_inputs(seed: int = 0) -> dict:
    arg_keys = jax.random.split(jax.random.key(seed), 9)
    return {
        "block_input": noise_with(arg_keys[0], (TOKENS, D), 1.0, 6.0, ((0, 16),), (0, 1, 16, 2.0)),
        "value_weight": bell_draw(arg_keys[1], (D, HEADS * HEAD), D ** -0.5, 0.09375, ((1, 8),)),
        "key_rows": bell_draw(arg_keys[2], (TOKENS, GROUPS * STATE), 0.125, 1.0, ((0, 16), (1, 8))),
        "query_rows": bell_draw(arg_keys[3], (TOKENS, GROUPS * STATE), 0.125, 1.0, ((0, 16), (1, 8))),
        "decay_pre": draw_decay_pre(jax.random.fold_in(arg_keys[8], 71), 0),
        "decay_log": draw_decay_log(jax.random.fold_in(arg_keys[8], 71), 0),
        "gate_rows": bell_draw(arg_keys[6], (TOKENS, HEADS * HEAD), 1.0, 6.0, ((0, 16), (1, 8))),
        "out_grad": bell_draw(arg_keys[7], (TOKENS, HEADS * HEAD), 1.0, 6.0, ((0, 16), (1, 8))),
    }


HIGH = lax.Precision.HIGHEST

def block_mixer(values, key_float, query_float, step_sizes, log_steps, start_state):
    length, head_count, head_width = values.shape
    groups = key_float.shape[1]
    group_ratio = head_count // groups
    blocks = length // BLK
    value_blocks = values.reshape(blocks, BLK, head_count, head_width)
    key_blocks = jnp.repeat(key_float.reshape(blocks, BLK, groups, -1), group_ratio, axis=2)
    query_blocks = jnp.repeat(query_float.reshape(blocks, BLK, groups, -1), group_ratio, axis=2)
    step_blocks = step_sizes.reshape(head_count, blocks, BLK).transpose(1, 0, 2)
    running = jnp.cumsum(log_steps.reshape(head_count, blocks, BLK).transpose(1, 0, 2), axis=-1)
    lower = jnp.tril(jnp.ones((BLK, BLK), bool))
    spread = jnp.where(lower, running[..., :, None] - running[..., None, :], 0.0)
    decay = jnp.where(lower, jnp.exp(spread), 0.0)
    scores = jnp.einsum('cqhn,ckhn->chqk', query_blocks, key_blocks, precision=HIGH)
    weights = scores * decay * step_blocks[:, :, None, :]
    inner = jnp.einsum('chqk,ckhp->cqhp', weights, value_blocks, precision=HIGH)
    to_end = jnp.exp(running[..., -1:] - running) * step_blocks
    block_states = jnp.einsum('cqhn,chq,cqhp->chpn', key_blocks, to_end, value_blocks, precision=HIGH)
    factors = jnp.exp(running[..., -1])

    def advance(state_now, item):
        contrib, factor = item
        return (factor[:, None, None] * state_now + contrib, state_now)
    end_state, before = lax.scan(advance, start_state, (block_states, factors))
    outer = jnp.einsum('cqhn,chpn,chq->cqhp', query_blocks, before, jnp.exp(running), precision=HIGH)
    return ((inner + outer).reshape(length, head_count, head_width), end_state)

def reference(block_input, value_weight, key_rows, query_rows, decay_pre, decay_log, gate_rows, out_grad):
    head_count = decay_log.shape[0]
    length = block_input.shape[0]
    groups = key_rows.shape[1] // STATE
    projected = jnp.dot(block_input, value_weight, preferred_element_type=jnp.float32).astype(jnp.bfloat16)
    pre_float = lax.optimization_barrier(projected).astype(jnp.float32)
    sig_pre = jax.nn.sigmoid(pre_float)
    values = (pre_float * sig_pre).reshape(length, head_count, HEAD)
    step_sizes = jax.nn.softplus(decay_pre)
    decay_rates = jnp.exp(decay_log)
    log_steps = -decay_rates[:, None] * step_sizes
    key_float = key_rows.astype(jnp.float32).reshape(length, groups, STATE)
    query_float = query_rows.astype(jnp.float32).reshape(length, groups, STATE)
    gate_float = gate_rows.astype(jnp.float32)
    sig_gate = jax.nn.sigmoid(gate_float)
    cot_float = out_grad.astype(jnp.float32)
    zero_state = jnp.zeros((head_count, HEAD, STATE), jnp.float32)

    def forward(vals, krows, qrows, sizes, logs):
        mixed, _ = block_mixer(vals, krows, qrows, sizes, logs, zero_state)
        return mixed
    mixed, pullback = jax.vjp(forward, values, key_float, query_float, step_sizes, log_steps)
    grad_mixed = (cot_float * gate_float * sig_gate).reshape(length, head_count, HEAD)
    value_back, key_back, query_back, size_back, log_back = pullback(grad_mixed)
    gate_grad = cot_float * mixed.reshape(length, head_count * HEAD) * sig_gate * (1.0 + gate_float * (1.0 - sig_gate))
    size_total = size_back - decay_rates[:, None] * log_back
    decay_grad = size_total * jax.nn.sigmoid(decay_pre)
    value_grad = (value_back.reshape(length, head_count * HEAD) * sig_pre * (1.0 + pre_float * (1.0 - sig_pre))).astype(jnp.bfloat16)
    weight_grad = lax.dot_general(block_input, value_grad, (((0,), (0,)), ((), ())), preferred_element_type=jnp.float32)
    row_norms = lax.optimization_barrier(jnp.sum(weight_grad * weight_grad, axis=1))
    return (key_back.reshape(length, groups * STATE), query_back.reshape(length, groups * STATE), decay_grad, gate_grad, weight_grad, row_norms)
```

```python
import functools

import jax
import jax.numpy as jnp
from jax import lax
from jax.experimental import pallas as pl
from jax.experimental.pallas import tpu as pltpu
from jax.sharding import PartitionSpec as P

HEAD = 64
STATE = 64
BLK = 128
RING = 4
F32 = jnp.float32
BF16 = jnp.bfloat16
HIGHEST = lax.Precision.HIGHEST
MESH = pl.DeviceIdType.MESH

ORDER = [
    (2, 2), (2, 0), (0, 2), (2, 1), (1, 2), (2, 3), (3, 2), (1, 3),
    (3, 1), (3, 3), (1, 1), (1, 0), (0, 1), (3, 0), (0, 3), (0, 0),
]


def nn(a, b, precision=None):
    return lax.dot_general(a, b, (((1,), (0,)), ((), ())), precision=precision, preferred_element_type=F32)


def nt(a, b, precision=None):
    return lax.dot_general(a, b, (((1,), (1,)), ((), ())), precision=precision, preferred_element_type=F32)


def tn(a, b, precision=None):
    return lax.dot_general(a, b, (((0,), (0,)), ((), ())), precision=precision, preferred_element_type=F32)


def halves(a):
    high = a.astype(BF16)
    return high, (a - high.astype(F32)).astype(BF16)


def both(a):
    return jnp.concatenate(halves(a), axis=1)


def folded(a):
    width = a.shape[1] // 2
    return a[:, :width] + a[:, width:]


def softplus(a):
    return jnp.maximum(a, 0.0) + jnp.log1p(jnp.exp(-jnp.abs(a)))


def sigmoid(a):
    return 1.0 / (1.0 + jnp.exp(-a))


def mixer(
    sp_count,
    tp_count,
    x_hbm, w_hbm, k_hbm, q_hbm, pre_hbm, rate_ref, gate_hbm, cot_hbm,
    kg_ref, qg_ref, dg_ref, gg_ref, wg_ref, rn_ref,
    x_v, w_v, k_v, q_v, pre_v, gate_v, cot_v,
    rows_s, stack_s, rend_s,
    dy_s, tm_s, lm_s, er_s, te_s, se_s, p_s, v_s, u_s,
    gst_s, sst_s, bs_s, out_s, inc_s, vgt_s,
    yy_s, dd_s, ee_s,
    gmsg, smsg, gslots, sslots,
    part, far_r, near_r, red_s, far2_r, near2_r,
    nmsg, nslots,
    in_sem, x_sem, gs_sem, gr_sem, ss_sem, sr_sem,
    fs_sem, fr_sem, ns_sem, nr_sem, f2s_sem, f2r_sem, n2s_sem, n2r_sem, norm_s, norm_r,
):
    tokens, width = x_v.shape
    blocks = tokens // BLK
    lanes = 2 * HEAD
    cols = width // sp_count
    me = lax.axis_index("sp")
    my_tp = lax.axis_index("tp")
    mz, mx = lax.div(me, RING), lax.rem(me, RING)

    barrier = pltpu.get_barrier_semaphore()
    for off in range(1, sp_count):
        pl.semaphore_signal(
            barrier, inc=1, device_id={"sp": lax.rem(me + off, sp_count)}, device_id_type=MESH
        )
    for off in range(1, tp_count):
        pl.semaphore_signal(
            barrier, inc=1, device_id={"tp": lax.rem(my_tp + off, tp_count)}, device_id_type=MESH
        )

    small = [
        pltpu.make_async_copy(src, dst, in_sem.at[i])
        for i, (src, dst) in enumerate(
            [(pre_hbm, pre_v), (q_hbm, q_v), (k_hbm, k_v), (gate_hbm, gate_v), (cot_hbm, cot_v), (w_hbm, w_v)]
        )
    ]
    for copy in small:
        copy.start()
    xrows = 2 * BLK
    xchunks = tokens // xrows

    def x_copy(i):
        rows = pl.ds(pl.multiple_of(i * xrows, xrows), xrows)
        return pltpu.make_async_copy(x_hbm.at[rows], x_v.at[rows], x_sem.at[i])

    for i in range(xchunks):
        x_copy(i).start()

    small[0].wait()
    for h in range(2):
        for c in range(blocks):
            rows_s[h * blocks + c : h * blocks + c + 1, :] = pre_v[h : h + 1, c * BLK : (c + 1) * BLK]
    pre = rows_s[...]
    row_id = lax.broadcasted_iota(jnp.int32, (2 * blocks, BLK), 0)
    rate = jnp.where(
        row_id < blocks,
        jnp.exp(jnp.full((2 * blocks, BLK), rate_ref[0], F32)),
        jnp.exp(jnp.full((2 * blocks, BLK), rate_ref[1], F32)),
    )
    step = softplus(pre)
    sq_row = lax.broadcasted_iota(jnp.int32, (BLK, BLK), 0)
    sq_col = lax.broadcasted_iota(jnp.int32, (BLK, BLK), 1)
    lower = sq_row >= sq_col
    run = nn(-rate * step, (sq_row <= sq_col).astype(F32), HIGHEST)
    stack_s[...] = jnp.zeros_like(stack_s)
    stack_s[0 : 2 * blocks, :] = run
    stack_s[2 * blocks : 4 * blocks, :] = step
    turned = stack_s[...].T
    first_head = lax.broadcasted_iota(jnp.int32, (BLK, lanes), 1) < HEAD
    first_lane = lax.broadcasted_iota(jnp.int32, (STATE, lanes), 1) < HEAD
    for copy in small[1:5]:
        copy.wait()

    def prepare(c, carry):
        rows = pl.ds(pl.multiple_of(c * BLK, BLK), BLK)
        rolled = pltpu.roll(turned, lax.rem(BLK - c, BLK), 1)
        col = [jnp.broadcast_to(rolled[:, i * blocks : i * blocks + 1], (BLK, BLK)) for i in range(4)]
        scores = nt(q_v[rows, :], k_v[rows, :])
        for h in range(2):
            row = stack_s[pl.ds(h * blocks + c, 1), :]
            decay = jnp.exp(jnp.where(lower, col[h] - row, -1e30))
            lm_s[rows, h * BLK : (h + 1) * BLK] = decay
            tm_s[rows, h * BLK : (h + 1) * BLK] = scores * decay
        running = jnp.where(first_head, col[0], col[1])
        end = running[BLK - 1 : BLK, :]
        er = jnp.exp(running)
        er_s[rows, :] = er
        te_s[rows, :] = jnp.exp(end - running)
        se_s[rows, :] = jnp.where(first_head, col[2], col[3])
        rend_s[pl.ds(c, 1), :] = end
        gate = gate_v[rows, :].astype(F32)
        dy = cot_v[rows, :].astype(F32) * gate * sigmoid(gate)
        dy_s[rows, :] = dy
        bs_s[c] = folded(tn(q_v[rows, :], both(er * dy)))
        return carry

    lax.fori_loop(0, blocks, prepare, 0)
    grad = jnp.zeros((STATE, lanes), F32)
    total = jnp.zeros((1, lanes), F32)
    for c in reversed(range(blocks)):
        end = rend_s[c : c + 1, :]
        grad = jnp.exp(end) * grad + bs_s[c]
        total = total + end
        gst_s[c] = grad
    gmsg[0:STATE, :] = grad
    gmsg[STATE : STATE + 8, :] = jnp.broadcast_to(total, (8, lanes))

    def state_copy(msg, slots, send, recv, source, target):
        return pltpu.make_async_remote_copy(
            src_ref=msg,
            dst_ref=slots.at[source],
            send_sem=send.at[target],
            recv_sem=recv.at[source],
            device_id={"sp": target},
            device_id_type=MESH,
        )

    pl.semaphore_wait(barrier, sp_count + tp_count - 2)
    for target in range(sp_count - 1):

        @pl.when(target < me)
        def _(target=target):
            state_copy(gmsg, gslots, gs_sem, gr_sem, me, target).start()

    small[5].wait()

    def project(i, carry):
        x_copy(i).wait()
        rows = pl.ds(pl.multiple_of(i * xrows, xrows), xrows)
        projected = nn(x_v[rows, :], w_v[...]).astype(BF16).astype(F32)
        p_s[rows, :] = projected
        v_s[rows, :] = projected * sigmoid(projected)
        for b in range(xrows // BLK):
            c = i * (xrows // BLK) + b
            rows = pl.ds(pl.multiple_of(c * BLK, BLK), BLK)
            bs_s[c] = folded(tn(k_v[rows, :], both(te_s[rows, :] * se_s[rows, :] * v_s[rows, :])))
            dy_high, dy_low = halves(dy_s[rows, :])
            t_high, t_low = halves(tm_s[rows, :])
            u = folded(tn(t_high, jnp.concatenate([dy_high, dy_low], axis=1))) + tn(t_low, dy_high)
            u_s[rows, :] = jnp.where(first_head, u[0:BLK, :], u[BLK : 2 * BLK, :])
        return carry

    lax.fori_loop(0, xchunks, project, 0)
    state = jnp.zeros((STATE, lanes), F32)
    for c in range(blocks):
        sst_s[c] = state
        state = jnp.exp(rend_s[c : c + 1, :]) * state + bs_s[c]
    smsg[0:STATE, :] = state
    smsg[STATE : STATE + 8, :] = jnp.broadcast_to(total, (8, lanes))
    for target in range(1, sp_count):

        @pl.when(target > me)
        def _(target=target):
            state_copy(smsg, sslots, ss_sem, sr_sem, me, target).start()

    out_s[...] = jnp.zeros_like(out_s)
    for source in reversed(range(1, sp_count)):

        @pl.when(source > me)
        def _(source=source):
            state_copy(gmsg, gslots, gs_sem, gr_sem, source, me).wait_recv()
            out_s[...] = gslots[source, 0:STATE, :] + jnp.exp(gslots[source, STATE : STATE + 1, :]) * out_s[...]

    after = jnp.zeros((1, lanes), F32)
    for c in reversed(range(blocks)):
        after = after + rend_s[c : c + 1, :]
        gst_s[c] = gst_s[c] + jnp.exp(after) * out_s[...]
    gst_s[blocks] = out_s[...]

    def value_gradient(c, carry):
        rows = pl.ds(pl.multiple_of(c * BLK, BLK), BLK)
        u = u_s[rows, :] + te_s[rows, :] * folded(nn(k_v[rows, :], both(gst_s[c + 1])))
        u_s[rows, :] = u
        projected = p_s[rows, :]
        sig = sigmoid(projected)
        vg = se_s[rows, :] * u * sig * (1.0 + projected * (1.0 - sig))
        vgt_s[:, rows] = vg.T.astype(BF16)
        return carry

    lax.fori_loop(0, blocks, value_gradient, 0)

    def owner(dz, dx):
        return lax.rem(mz + dz, RING) * RING + lax.rem(mx + dx, RING)

    def neighbour(half, stage, direction):
        if half == stage:
            return lax.rem(mz + direction + RING, RING) * RING + mx
        return mz * RING + lax.rem(mx + direction + RING, RING)

    def half_of(half, dz, dx):
        return part.at[owner(dz, dx), half * HEAD : (half + 1) * HEAD, :]

    def piece(half, dist, across):
        return half_of(half, dist, across) if half == 0 else half_of(half, across, dist)

    def far_copy(half, across):
        direction = 1 if across < 2 else -1
        slot = half * RING + across
        return pltpu.make_async_remote_copy(
            src_ref=piece(half, 2, across),
            dst_ref=far_r.at[slot],
            send_sem=fs_sem.at[slot],
            recv_sem=fr_sem.at[slot],
            device_id={"sp": neighbour(half, 0, direction)},
            device_id_type=MESH,
        )

    def near_copy(half, direction, across):
        slot = (half * 2 + (0 if direction == 1 else 1)) * RING + across
        return pltpu.make_async_remote_copy(
            src_ref=piece(half, 1 if direction == 1 else 3, across),
            dst_ref=near_r.at[slot],
            send_sem=ns_sem.at[slot],
            recv_sem=nr_sem.at[slot],
            device_id={"sp": neighbour(half, 0, direction)},
            device_id_type=MESH,
        )

    for dz, dx in ORDER:
        dest = owner(dz, dx)
        columns = pl.ds(pl.multiple_of(dest * cols, cols), cols)
        part[dest] = nn(vgt_s[...], x_v[:, columns])
        for half, dist, across in ((0, dz, dx), (1, dx, dz)):
            if dist == 2:
                far_copy(half, across).start()
            elif dist == 1 and across >= 2:
                near_copy(half, 1, across).start()
            elif dist == 3 and across < 2:
                near_copy(half, -1, across).start()
    for across in range(2):
        for half in range(2):
            for direction, lane in ((1, across), (-1, across + 2)):
                far_copy(half, lane).wait_recv()
                ref = piece(half, 1 if direction == 1 else 3, lane)
                ref[...] = ref[...] + far_r[half * RING + lane]
                near_copy(half, direction, lane).start()

    inc_s[...] = jnp.zeros_like(inc_s)
    for source in range(sp_count - 1):

        @pl.when(source < me)
        def _(source=source):
            state_copy(smsg, sslots, ss_sem, sr_sem, source, me).wait_recv()
            inc_s[...] = sslots[source, 0:STATE, :] + jnp.exp(sslots[source, STATE : STATE + 1, :]) * inc_s[...]

    before = jnp.zeros((1, lanes), F32)
    for c in range(blocks):
        full = sst_s[c] + jnp.exp(before) * inc_s[...]
        sst_s[c] = full
        before = before + rend_s[c : c + 1, :]
        if c > 0:
            ee_s[c - 1 : c, :] = jnp.sum(full * gst_s[c], axis=0, keepdims=True)
    last = smsg[0:STATE, :] + jnp.exp(before) * inc_s[...]
    ee_s[blocks - 1 : blocks, :] = jnp.sum(last * gst_s[blocks], axis=0, keepdims=True)

    head_of = lax.broadcasted_iota(jnp.int32, (8, lanes), 0)
    lane_head = lax.div(lax.broadcasted_iota(jnp.int32, (8, lanes), 1), HEAD)
    pick = (head_of == lane_head).astype(BF16)
    zero = jnp.zeros((BLK, lanes), BF16)

    def head_rows(a):
        high, low = halves(a)
        return nt(pick, high) + nt(pick, low)

    def others(c, carry):
        rows = pl.ds(pl.multiple_of(c * BLK, BLK), BLK)
        q, k = q_v[rows, :], k_v[rows, :]
        dy, v, u, er, te = dy_s[rows, :], v_s[rows, :], u_s[rows, :], er_s[rows, :], te_s[rows, :]
        sv = se_s[rows, :] * v
        sv_high, sv_low = halves(sv)
        dy_high, dy_low = halves(dy)

        def split_heads(a, axis):
            return jnp.concatenate([jnp.where(first_head, a, zero), jnp.where(first_head, zero, a)], axis=axis)

        t_high, t_low = halves(tm_s[rows, :])
        spread_high = split_heads(sv_high, 0)
        mixed = folded(nn(t_high, jnp.concatenate([spread_high, split_heads(sv_low, 0)], axis=1)))
        mixed = mixed + nn(t_low, spread_high)
        mixed = mixed + er * folded(nn(q, both(sst_s[c])))
        gate = gate_v[rows, :].astype(F32)
        sig = sigmoid(gate)
        gg_ref[rows, :] = cot_v[rows, :].astype(F32) * mixed * sig * (1.0 + gate * (1.0 - sig))
        by_head = split_heads(dy_high, 0)
        dp = nt(jnp.concatenate([by_head, split_heads(dy_low, 0)], axis=1), jnp.concatenate([sv_high, sv_high], axis=1))
        dp = dp + nt(by_head, sv_low)
        d = dp[0:BLK, :] * lm_s[rows, 0:BLK] + dp[BLK : 2 * BLK, :] * lm_s[rows, BLK : 2 * BLK]
        d_high, d_low = halves(d)
        es_high, es_low = halves(er * dy)
        s_high, s_low = halves(sst_s[c])
        qg_ref[rows, :] = (
            nn(d_high, k) + nn(d_low, k) + nt(es_high, s_high) + nt(es_low, s_high) + nt(es_high, s_low)
        )
        ts_high, ts_low = halves(te * sv)
        g_high, g_low = halves(gst_s[c + 1])
        kg_ref[rows, :] = (
            tn(d_high, q) + tn(d_low, q) + nt(ts_high, g_high) + nt(ts_low, g_high) + nt(ts_high, g_low)
        )
        yy = head_rows(dy * mixed)
        dd = head_rows(v * u)
        for h in range(2):
            yy_s[pl.ds(h * blocks + c, 1), :] = yy[h : h + 1, :]
            dd_s[pl.ds(h * blocks + c, 1), :] = dd[h : h + 1, :]
        return carry

    half_way = blocks // 2
    lax.fori_loop(0, half_way, others, 0)

    quarter = HEAD // 2

    def total_of(half, across):
        plus, minus = (half * 2) * RING + across, (half * 2 + 1) * RING + across
        near_copy(half, 1, across).wait_recv()
        near_copy(half, -1, across).wait_recv()
        return piece(half, 0, across)[...] + near_r[plus] + near_r[minus]

    def far2_copy(half, which):
        slot = half * 2 + which
        return pltpu.make_async_remote_copy(
            src_ref=red_s.at[half * RING + 2, which * quarter : (which + 1) * quarter, :],
            dst_ref=far2_r.at[slot],
            send_sem=f2s_sem.at[slot],
            recv_sem=f2r_sem.at[slot],
            device_id={"sp": neighbour(half, 1, 1 if which == 0 else -1)},
            device_id_type=MESH,
        )

    def near2_copy(half, direction, which):
        side = 0 if direction == 1 else 1
        slot = (half * 2 + side) * 2 + which
        return pltpu.make_async_remote_copy(
            src_ref=red_s.at[half * RING + (1 if direction == 1 else 3), which * quarter : (which + 1) * quarter, :],
            dst_ref=near2_r.at[slot],
            send_sem=n2s_sem.at[slot],
            recv_sem=n2r_sem.at[slot],
            device_id={"sp": neighbour(half, 1, direction)},
            device_id_type=MESH,
        )

    for across in (2, 1, 3, 0):
        for half in range(2):
            red_s[half * RING + across] = total_of(half, across)
            if across == 2:
                far2_copy(half, 0).start()
                far2_copy(half, 1).start()
            elif across == 1:
                near2_copy(half, 1, 1).start()
            elif across == 3:
                near2_copy(half, -1, 0).start()
    for half in range(2):
        for direction, which in ((1, 0), (-1, 1)):
            far2_copy(half, which).wait_recv()
            at = half * RING + (1 if direction == 1 else 3)
            span = slice(which * quarter, (which + 1) * quarter)
            red_s[at, span, :] = red_s[at, span, :] + far2_r[half * 2 + which]
            near2_copy(half, direction, which).start()

    lax.fori_loop(half_way, blocks, others, 0)

    ends = ee_s[...]
    end_cols = jnp.concatenate(
        [
            jnp.sum(ends[:, 0:HEAD], axis=1, keepdims=True),
            jnp.sum(ends[:, HEAD:lanes], axis=1, keepdims=True),
        ],
        axis=0,
    )
    direct = dd_s[...]
    log_grad = nn(yy_s[...] - step * direct, lower.astype(F32), HIGHEST) + end_cols
    decay_grad = (direct - rate * log_grad) * sigmoid(pre)
    for h in range(2):
        for c in range(blocks):
            dg_ref[h : h + 1, c * BLK : (c + 1) * BLK] = decay_grad[h * blocks + c : h * blocks + c + 1, :]

    squares = jnp.zeros((1, cols), F32)
    for half in range(2):
        for which in range(2):
            for direction in (1, -1):
                near2_copy(half, direction, which).wait_recv()
            plus, minus = (half * 2) * 2 + which, (half * 2 + 1) * 2 + which
            span = slice(which * quarter, (which + 1) * quarter)
            done = red_s[half * RING, span, :] + near2_r[plus] + near2_r[minus]
            red_s[half * RING, span, :] = done
            squares = squares + jnp.sum(done * done, axis=0, keepdims=True)

    def norm_copy(source, target):
        return pltpu.make_async_remote_copy(
            src_ref=nmsg,
            dst_ref=nslots.at[source],
            send_sem=norm_s.at[target],
            recv_sem=norm_r.at[source],
            device_id={"tp": target},
            device_id_type=MESH,
        )

    nmsg[...] = jnp.broadcast_to(squares, (8, cols))
    for off in range(1, tp_count):
        norm_copy(my_tp, lax.rem(my_tp + off, tp_count)).start()
    for half in range(2):
        wg_ref[:, half * HEAD : (half + 1) * HEAD] = red_s[half * RING].T
    norms = squares
    for off in range(1, tp_count):
        source = lax.rem(my_tp + off, tp_count)
        norm_copy(source, my_tp).wait_recv()
        norms = norms + nslots[source, 0:1, :]
    rn_ref[...] = norms

    for target in range(sp_count - 1):

        @pl.when(target < me)
        def _(target=target):
            state_copy(gmsg, gslots, gs_sem, gr_sem, me, target).wait_send()

    for target in range(1, sp_count):

        @pl.when(target > me)
        def _(target=target):
            state_copy(smsg, sslots, ss_sem, sr_sem, me, target).wait_send()

    for half in range(2):
        for across in range(RING):
            far_copy(half, across).wait_send()
            for direction in (1, -1):
                near_copy(half, direction, across).wait_send()
        for which in range(2):
            far2_copy(half, which).wait_send()
            for direction in (1, -1):
                near2_copy(half, direction, which).wait_send()
    for off in range(1, tp_count):
        norm_copy(my_tp, lax.rem(my_tp + off, tp_count)).wait_send()


def shards(sp_count, tp_count, block_input, value_weight, key_rows, query_rows, decay_pre, decay_log, gate_rows, out_grad):
    tokens, width = block_input.shape
    blocks = tokens // BLK
    lanes = 2 * HEAD
    cols = width // sp_count
    vmem = lambda shape, dtype=F32: pltpu.VMEM(shape, dtype)
    dma = lambda *shape: pltpu.SemaphoreType.DMA(shape)
    state_msg = (STATE + 8, lanes)
    scratch = [
        vmem((tokens, width), BF16), vmem((width, lanes), BF16), vmem((tokens, STATE), BF16), vmem((tokens, STATE), BF16),
        vmem((2, tokens)), vmem((tokens, lanes), BF16), vmem((tokens, lanes), BF16),
        vmem((2 * blocks, BLK)), vmem((BLK, BLK)), vmem((blocks, lanes)),
        vmem((tokens, lanes)), vmem((tokens, 2 * BLK)), vmem((tokens, 2 * BLK)), vmem((tokens, lanes)),
        vmem((tokens, lanes)), vmem((tokens, lanes)), vmem((tokens, lanes)), vmem((tokens, lanes)), vmem((tokens, lanes)),
        vmem((blocks + 1, STATE, lanes)), vmem((blocks, STATE, lanes)), vmem((blocks, STATE, lanes)),
        vmem((STATE, lanes)), vmem((STATE, lanes)), vmem((lanes, tokens), BF16),
        vmem((2 * blocks, BLK)), vmem((2 * blocks, BLK)), vmem((blocks, lanes)),
        vmem(state_msg), vmem(state_msg), vmem((sp_count, *state_msg)), vmem((sp_count, *state_msg)),
        vmem((sp_count, lanes, cols)), vmem((8, HEAD, cols)), vmem((16, HEAD, cols)), vmem((8, HEAD, cols)),
        vmem((4, HEAD // 2, cols)), vmem((8, HEAD // 2, cols)),
        vmem((8, cols)), vmem((tp_count, 8, cols)),
        dma(6), dma(tokens // (2 * BLK)), dma(sp_count), dma(sp_count), dma(sp_count), dma(sp_count),
        dma(8), dma(8), dma(16), dma(16), dma(4), dma(4), dma(8), dma(8), dma(tp_count), dma(tp_count),
    ]
    hbm = pl.BlockSpec(memory_space=pl.ANY)
    in_vmem = pl.BlockSpec(memory_space=pltpu.VMEM)
    outs = pl.pallas_call(
        functools.partial(mixer, sp_count, tp_count),
        out_shape=(
            jax.ShapeDtypeStruct((tokens, STATE), F32),
            jax.ShapeDtypeStruct((tokens, STATE), F32),
            jax.ShapeDtypeStruct((2, tokens), F32),
            jax.ShapeDtypeStruct((tokens, lanes), F32),
            jax.ShapeDtypeStruct((cols, lanes), F32),
            jax.ShapeDtypeStruct((1, cols), F32),
        ),
        in_specs=[hbm, hbm, hbm, hbm, hbm, pl.BlockSpec(memory_space=pltpu.SMEM), hbm, hbm],
        out_specs=tuple([in_vmem] * 6),
        scratch_shapes=scratch,
        compiler_params=pltpu.CompilerParams(
            collective_id=0, has_side_effects=True, vmem_limit_bytes=60 * 1024 * 1024
        ),
        name="mixer",
    )(block_input, value_weight, key_rows, query_rows, decay_pre, decay_log, gate_rows, out_grad)
    return (*outs[:5], outs[5].reshape(cols))


def solution(mesh):
    in_specs = (
        P("sp", None),
        P(None, "tp"),
        P("sp", "tp"),
        P("sp", "tp"),
        P("tp", "sp"),
        P("tp"),
        P("sp", "tp"),
        P("sp", "tp"),
    )
    out_specs = (P("sp", "tp"), P("sp", "tp"), P("tp", "sp"), P("sp", "tp"), P("sp", "tp"), P("sp"))
    body = functools.partial(shards, mesh.shape["sp"], mesh.shape["tp"])
    return jax.shard_map(body, mesh=mesh, in_specs=in_specs, out_specs=out_specs, check_vma=False)
```

```python
import functools

import jax
import jax.numpy as jnp
from jax import lax
from jax.experimental import pallas as pl
from jax.experimental.pallas import tpu as pltpu
from jax.sharding import PartitionSpec as P

HEAD = 64
STATE = 64
BLK = 128
RING = 4
F32 = jnp.float32
BF16 = jnp.bfloat16
HIGHEST = lax.Precision.HIGHEST
MESH = pl.DeviceIdType.MESH

ORDER = [
    [(2, 2)], [(2, 0), (0, 2)], [(2, 1), (1, 2)], [(2, 3), (3, 2)], [(1, 3), (3, 1)],
    [(3, 3), (1, 1)], [(1, 0), (0, 1)], [(3, 0), (0, 3)], [(0, 0)],
]


def nn(a, b, precision=None):
    return lax.dot_general(a, b, (((1,), (0,)), ((), ())), precision=precision, preferred_element_type=F32)


def nt(a, b, precision=None):
    return lax.dot_general(a, b, (((1,), (1,)), ((), ())), precision=precision, preferred_element_type=F32)


def tn(a, b, precision=None):
    return lax.dot_general(a, b, (((0,), (0,)), ((), ())), precision=precision, preferred_element_type=F32)


def halves(a):
    high = a.astype(BF16)
    return high, (a - high.astype(F32)).astype(BF16)


def both(a):
    return jnp.concatenate(halves(a), axis=1)


def folded(a):
    width = a.shape[1] // 2
    return a[:, :width] + a[:, width:]


def softplus(a):
    return jnp.maximum(a, 0.0) + jnp.log1p(jnp.exp(-jnp.abs(a)))


def sigmoid(a):
    return 1.0 / (1.0 + jnp.exp(-a))


def mixer(
    sp_count,
    tp_count,
    x_hbm, w_hbm, k_hbm, q_hbm, pre_hbm, rate_hbm, gate_hbm, cot_hbm,
    kg_ref, qg_ref, dg_ref, gg_ref, wg_ref, rn_ref,
    x_v, w_v, k_v, q_v, pre_v, rate_ref, gate_v, cot_v,
    rows_s, stack_s, rend_s,
    dy_s, tm_s, lm_s, er_s, te_s, se_s, p_s, v_s, u_s,
    gst_s, sst_s, bs_s, out_s, inc_s, vgt_s,
    yy_s, dd_s, ee_s,
    last_s, grow, gcol, srow, scol,
    part, far_r, near_r, red_s, far2_r, near2_r,
    nmsg, nslots,
    in_sem, x_sem, gs_sem, gr_sem, ss_sem, sr_sem, gs2_sem, gr2_sem, ss2_sem, sr2_sem,
    fs_sem, fr_sem, ns_sem, nr_sem, f2s_sem, f2r_sem, n2s_sem, n2r_sem, norm_s, norm_r,
):
    tokens, width = x_v.shape
    blocks = tokens // BLK
    lanes = 2 * HEAD
    cols = width // sp_count
    me = lax.axis_index("sp")
    my_tp = lax.axis_index("tp")
    mz, mx = lax.div(me, RING), lax.rem(me, RING)

    barrier = pltpu.get_barrier_semaphore()
    for off in range(1, RING):
        for peer in (mz * RING + lax.rem(mx + off, RING), lax.rem(mz + off, RING) * RING + mx):
            pl.semaphore_signal(barrier, inc=1, device_id={"sp": peer}, device_id_type=MESH)
    for off in range(1, tp_count):
        pl.semaphore_signal(
            barrier, inc=1, device_id={"tp": lax.rem(my_tp + off, tp_count)}, device_id_type=MESH
        )

    small = [
        pltpu.make_async_copy(src, dst, in_sem.at[i])
        for i, (src, dst) in enumerate(
            [
                (pre_hbm, pre_v), (rate_hbm, rate_ref), (gate_hbm, gate_v), (cot_hbm, cot_v), (q_hbm, q_v), (k_hbm, k_v), (w_hbm, w_v)
            ]
        )
    ]
    for copy in small:
        copy.start()
    xrows = tokens // x_sem.shape[0]
    xchunks = tokens // xrows

    def x_copy(i):
        rows = pl.ds(pl.multiple_of(i * xrows, xrows), xrows)
        return pltpu.make_async_copy(x_hbm.at[rows], x_v.at[rows], x_sem.at[i])

    small[0].wait()
    small[1].wait()
    for h in range(2):
        for c in range(blocks):
            rows_s[h * blocks + c : h * blocks + c + 1, :] = pre_v[h : h + 1, c * BLK : (c + 1) * BLK]
    pre = rows_s[...]
    row_id = lax.broadcasted_iota(jnp.int32, (2 * blocks, BLK), 0)
    rate = jnp.where(
        row_id < blocks,
        jnp.exp(jnp.full((2 * blocks, BLK), rate_ref[0], F32)),
        jnp.exp(jnp.full((2 * blocks, BLK), rate_ref[1], F32)),
    )
    step = softplus(pre)
    sq_row = lax.broadcasted_iota(jnp.int32, (BLK, BLK), 0)
    sq_col = lax.broadcasted_iota(jnp.int32, (BLK, BLK), 1)
    lower = sq_row >= sq_col
    run = nn(-rate * step, (sq_row <= sq_col).astype(F32), HIGHEST)
    stack_s[...] = jnp.zeros_like(stack_s)
    stack_s[0 : 2 * blocks, :] = run
    stack_s[2 * blocks : 4 * blocks, :] = step
    turned = stack_s[...].T
    first_head = lax.broadcasted_iota(jnp.int32, (BLK, lanes), 1) < HEAD
    for copy in small[2:6]:
        copy.wait()
    for i in range(xchunks):
        x_copy(i).start()

    def block_rows(c):
        return pl.ds(pl.multiple_of(c * BLK, BLK), BLK)

    def for_blocks(start, stop, unroll, body):
        def step_of(i, carry):
            for b in range(unroll):
                body(start + i * unroll + b)
            return carry

        lax.fori_loop(0, (stop - start) // unroll, step_of, 0)

    def columns_of(c, kinds):
        rolled = pltpu.roll(turned, lax.rem(BLK - c, BLK), 1)
        return [jnp.broadcast_to(rolled[:, i * blocks : i * blocks + 1], (BLK, BLK)) for i in kinds]

    def prepare(c):
        rows = block_rows(c)
        running = jnp.where(first_head, *columns_of(c, (0, 1)))
        er = jnp.exp(running)
        er_s[rows, :] = er
        rend_s[pl.ds(c, 1), :] = running[BLK - 1 : BLK, :]
        gate = gate_v[rows, :].astype(F32)
        dy = cot_v[rows, :].astype(F32) * gate * sigmoid(gate)
        dy_s[rows, :] = dy
        bs_s[c] = folded(nn(q_v[:, rows], both(er * dy)))

    for_blocks(0, blocks, min(4, blocks), prepare)
    grad = jnp.zeros((STATE, lanes), F32)
    total = jnp.zeros((1, lanes), F32)
    for c in reversed(range(blocks)):
        end = rend_s[c : c + 1, :]
        grad = jnp.exp(end) * grad + bs_s[c]
        total = total + end
        gst_s[c] = grad
    def message(ref, at, value, log):
        ref[at, 0:STATE, :] = value
        ref[at, STATE : STATE + 8, :] = jnp.broadcast_to(log, (8, lanes))

    def row_copy(slots, send, recv, source, target):
        return pltpu.make_async_remote_copy(
            src_ref=slots.at[source],
            dst_ref=slots.at[source],
            send_sem=send.at[target],
            recv_sem=recv.at[source],
            device_id={"sp": mz * RING + target},
            device_id_type=MESH,
        )

    def col_copy(slots, send, recv, source, target):
        return pltpu.make_async_remote_copy(
            src_ref=slots.at[source],
            dst_ref=slots.at[source],
            send_sem=send.at[target],
            recv_sem=recv.at[source],
            device_id={"sp": target * RING + mx},
            device_id_type=MESH,
        )

    def send_row(slots, send, recv):
        for off in range(1, RING):
            row_copy(slots, send, recv, mx, lax.rem(mx + off, RING)).start()

    def row_sum(slots, send, recv, order):
        for off in range(1, RING):
            row_copy(slots, send, recv, lax.rem(mx + off, RING), mx).wait_recv()
        acc = jnp.zeros((STATE, lanes), F32)
        log = jnp.zeros((1, lanes), F32)
        own, own_log = acc, log
        for at in order:
            own = jnp.where(mx == at, acc, own)
            own_log = jnp.where(mx == at, log, own_log)
            tail = slots[at, STATE : STATE + 1, :]
            acc = slots[at, 0:STATE, :] + jnp.exp(tail) * acc
            log = log + tail
        return own, own_log, acc, log

    message(grow, mx, grad, total)
    pl.semaphore_wait(barrier, 2 * (RING - 1) + tp_count - 1)
    send_row(grow, gs_sem, gr_sem)

    def project(i):
        x_copy(i).wait()
        rows = pl.ds(pl.multiple_of(i * xrows, xrows), xrows)
        p_s[rows, :] = nn(x_v[rows, :], w_v[...]).astype(BF16).astype(F32)

    def local(c):
        rows = block_rows(c)
        col = columns_of(c, range(4))
        scores = tn(q_v[:, rows], k_v[:, rows])
        weights = []
        for h in range(2):
            row = stack_s[pl.ds(h * blocks + c, 1), :]
            decay = jnp.exp(jnp.where(lower, col[h] - row, -1e30))
            lm_s[rows, h * BLK : (h + 1) * BLK] = decay
            weights.append(scores * decay)
        weights = jnp.concatenate(weights, axis=1)
        tm_s[rows, :] = weights
        running = jnp.where(first_head, col[0], col[1])
        te_s[rows, :] = jnp.exp(running[BLK - 1 : BLK, :] - running)
        se_s[rows, :] = jnp.where(first_head, col[2], col[3])
        dy_high, dy_low = halves(dy_s[rows, :])
        t_high, t_low = halves(weights)
        u = folded(tn(t_high, jnp.concatenate([dy_high, dy_low], axis=1))) + tn(t_low, dy_high)
        u_s[rows, :] = jnp.where(first_head, u[0:BLK, :], u[BLK : 2 * BLK, :])

    def with_values(c):
        rows = block_rows(c)
        projected = p_s[rows, :]
        v = projected * sigmoid(projected)
        v_s[rows, :] = v
        bs_s[c] = folded(nn(k_v[:, rows], both(te_s[rows, :] * se_s[rows, :] * v)))

    for_blocks(0, blocks, min(4, blocks), local)
    small[6].wait()

    def chunk(i, carry):
        project(i)
        return carry

    lax.fori_loop(0, xchunks // 2, chunk, 0)
    own_grad, own_log, ring_grad, ring_log = row_sum(grow, gs_sem, gr_sem, (3, 2, 1, 0))
    message(gcol, mz, ring_grad, ring_log)
    for target in range(RING - 1):

        @pl.when(target < mz)
        def _(target=target):
            col_copy(gcol, gs2_sem, gr2_sem, mz, target).start()

    lax.fori_loop(xchunks // 2, xchunks, chunk, 0)
    for_blocks(0, blocks, min(4, blocks), with_values)
    state = jnp.zeros((STATE, lanes), F32)
    for c in range(blocks):
        sst_s[c] = state
        state = jnp.exp(rend_s[c : c + 1, :]) * state + bs_s[c]
    last_s[...] = state
    message(srow, mx, state, total)
    send_row(srow, ss_sem, sr_sem)

    out_s[...] = jnp.zeros_like(out_s)
    for source in reversed(range(1, RING)):

        @pl.when(source > mz)
        def _(source=source):
            col_copy(gcol, gs2_sem, gr2_sem, source, mz).wait_recv()
            out_s[...] = gcol[source, 0:STATE, :] + jnp.exp(gcol[source, STATE : STATE + 1, :]) * out_s[...]

    out_s[...] = own_grad + jnp.exp(own_log) * out_s[...]
    after = jnp.zeros((1, lanes), F32)
    for c in reversed(range(blocks)):
        after = after + rend_s[c : c + 1, :]
        gst_s[c] = gst_s[c] + jnp.exp(after) * out_s[...]
    gst_s[blocks] = out_s[...]

    def value_gradient(c):
        rows = block_rows(c)
        u = u_s[rows, :] + te_s[rows, :] * folded(tn(k_v[:, rows], both(gst_s[c + 1])))
        u_s[rows, :] = u
        projected = p_s[rows, :]
        sig = sigmoid(projected)
        vg = se_s[rows, :] * u * sig * (1.0 + projected * (1.0 - sig))
        vgt_s[:, rows] = vg.astype(BF16).T

    for_blocks(0, blocks, min(4, blocks), value_gradient)

    def owner(dz, dx):
        return lax.rem(mz + dz, RING) * RING + lax.rem(mx + dx, RING)

    def neighbour(half, stage, direction):
        if half == stage:
            return lax.rem(mz + direction + RING, RING) * RING + mx
        return mz * RING + lax.rem(mx + direction + RING, RING)

    def half_of(half, dz, dx):
        return part.at[owner(dz, dx), half * HEAD : (half + 1) * HEAD, :]

    def piece(half, dist, across):
        return half_of(half, dist, across) if half == 0 else half_of(half, across, dist)

    def far_copy(half, across):
        direction = 1 if across < 2 else -1
        slot = half * RING + across
        return pltpu.make_async_remote_copy(
            src_ref=piece(half, 2, across),
            dst_ref=far_r.at[slot],
            send_sem=fs_sem.at[slot],
            recv_sem=fr_sem.at[slot],
            device_id={"sp": neighbour(half, 0, direction)},
            device_id_type=MESH,
        )

    def near_copy(half, direction, across):
        slot = (half * 2 + (0 if direction == 1 else 1)) * RING + across
        return pltpu.make_async_remote_copy(
            src_ref=piece(half, 1 if direction == 1 else 3, across),
            dst_ref=near_r.at[slot],
            send_sem=ns_sem.at[slot],
            recv_sem=nr_sem.at[slot],
            device_id={"sp": neighbour(half, 0, direction)},
            device_id_type=MESH,
        )

    for number, group in enumerate(ORDER):
        if number == 4:
            own_state, own_state_log, ring_state, ring_log = row_sum(srow, ss_sem, sr_sem, (0, 1, 2, 3))
            message(scol, mz, ring_state, ring_log)
            for target in range(1, RING):

                @pl.when(target > mz)
                def _(target=target):
                    col_copy(scol, ss2_sem, sr2_sem, mz, target).start()
        for dz, dx in group:
            dest = owner(dz, dx)
            columns = pl.ds(pl.multiple_of(dest * cols, cols), cols)
            part[dest] = nn(vgt_s[...], x_v[:, columns])
        for dz, dx in group:
            for half, dist, across in ((0, dz, dx), (1, dx, dz)):
                if dist == 2:
                    far_copy(half, across).start()
                elif dist == 1 and across >= 2:
                    near_copy(half, 1, across).start()
                elif dist == 3 and across < 2:
                    near_copy(half, -1, across).start()
    for across in range(2):
        for half in range(2):
            for direction, lane in ((1, across), (-1, across + 2)):
                far_copy(half, lane).wait_recv()
                ref = piece(half, 1 if direction == 1 else 3, lane)
                ref[...] = ref[...] + far_r[half * RING + lane]
                near_copy(half, direction, lane).start()

    inc_s[...] = jnp.zeros_like(inc_s)
    for source in range(RING - 1):

        @pl.when(source < mz)
        def _(source=source):
            col_copy(scol, ss2_sem, sr2_sem, source, mz).wait_recv()
            inc_s[...] = scol[source, 0:STATE, :] + jnp.exp(scol[source, STATE : STATE + 1, :]) * inc_s[...]

    inc_s[...] = own_state + jnp.exp(own_state_log) * inc_s[...]
    before = jnp.zeros((1, lanes), F32)
    for c in range(blocks):
        full = sst_s[c] + jnp.exp(before) * inc_s[...]
        sst_s[c] = full
        before = before + rend_s[c : c + 1, :]
        if c > 0:
            ee_s[c - 1 : c, :] = jnp.sum(full * gst_s[c], axis=0, keepdims=True)
    last = last_s[...] + jnp.exp(before) * inc_s[...]
    ee_s[blocks - 1 : blocks, :] = jnp.sum(last * gst_s[blocks], axis=0, keepdims=True)

    zero = jnp.zeros((BLK, lanes), BF16)
    lane_id = lax.broadcasted_iota(jnp.int32, (BLK, lanes), 1)
    yy_s[...] = jnp.zeros_like(yy_s)
    dd_s[...] = jnp.zeros_like(dd_s)

    def keep_head_sums(ref, c, a):
        first = jnp.sum(jnp.where(first_head, a, 0.0), axis=1, keepdims=True)
        second = jnp.sum(jnp.where(first_head, 0.0, a), axis=1, keepdims=True)
        ref[...] = jnp.where(lane_id == c, first, jnp.where(lane_id == blocks + c, second, ref[...]))

    def others(c):
        rows = block_rows(c)
        q, k = q_v[:, rows], k_v[:, rows]
        dy, v, u, er, te = dy_s[rows, :], v_s[rows, :], u_s[rows, :], er_s[rows, :], te_s[rows, :]
        sv = se_s[rows, :] * v
        sv_high, sv_low = halves(sv)

        def split_heads(a, axis):
            return jnp.concatenate([jnp.where(first_head, a, zero), jnp.where(first_head, zero, a)], axis=axis)

        spread = jnp.concatenate([split_heads(sv_high, 0), split_heads(sv_low, 0)], axis=1)
        mixed = folded(nn(tm_s[rows, :].astype(BF16), spread)) + er * folded(tn(q, both(sst_s[c])))
        gate = gate_v[rows, :].astype(F32)
        sig = sigmoid(gate)
        gg_ref[rows, :] = cot_v[rows, :].astype(F32) * mixed * sig * (1.0 + gate * (1.0 - sig))
        dp = nt(split_heads(dy.astype(BF16), 0), sv_high)
        d = dp[0:BLK, :] * lm_s[rows, 0:BLK] + dp[BLK : 2 * BLK, :] * lm_s[rows, BLK : 2 * BLK]
        d_high, d_low = halves(d)
        qg_ref[:, rows] = nt(
            jnp.concatenate([k, k], axis=1), jnp.concatenate([d_high, d_low], axis=1)
        ) + nt(sst_s[c].astype(BF16), (er * dy).astype(BF16))
        kg_ref[:, rows] = nn(
            jnp.concatenate([q, q], axis=1), jnp.concatenate([d_high, d_low], axis=0)
        ) + nt(gst_s[c + 1].astype(BF16), (te * sv).astype(BF16))
        keep_head_sums(yy_s, c, dy * mixed)
        keep_head_sums(dd_s, c, v * u)

    for_blocks(0, blocks, 2, others)
    ends = ee_s[...]
    end_cols = jnp.concatenate(
        [
            jnp.sum(ends[:, 0:HEAD], axis=1, keepdims=True),
            jnp.sum(ends[:, HEAD:lanes], axis=1, keepdims=True),
        ],
        axis=0,
    )
    direct = dd_s[...].T[0 : 2 * blocks, :]
    log_grad = nn(yy_s[...].T[0 : 2 * blocks, :] - step * direct, lower.astype(F32), HIGHEST) + end_cols
    decay_grad = (direct - rate * log_grad) * sigmoid(pre)
    for h in range(2):
        for c in range(blocks):
            dg_ref[h : h + 1, c * BLK : (c + 1) * BLK] = decay_grad[h * blocks + c : h * blocks + c + 1, :]

    quarter = HEAD // 2

    def total_of(half, across):
        plus, minus = (half * 2) * RING + across, (half * 2 + 1) * RING + across
        near_copy(half, 1, across).wait_recv()
        near_copy(half, -1, across).wait_recv()
        return piece(half, 0, across)[...] + near_r[plus] + near_r[minus]

    def far2_copy(half, which):
        slot = half * 2 + which
        return pltpu.make_async_remote_copy(
            src_ref=red_s.at[half * RING + 2, which * quarter : (which + 1) * quarter, :],
            dst_ref=far2_r.at[slot],
            send_sem=f2s_sem.at[slot],
            recv_sem=f2r_sem.at[slot],
            device_id={"sp": neighbour(half, 1, 1 if which == 0 else -1)},
            device_id_type=MESH,
        )

    def near2_copy(half, direction, which):
        side = 0 if direction == 1 else 1
        slot = (half * 2 + side) * 2 + which
        return pltpu.make_async_remote_copy(
            src_ref=red_s.at[half * RING + (1 if direction == 1 else 3), which * quarter : (which + 1) * quarter, :],
            dst_ref=near2_r.at[slot],
            send_sem=n2s_sem.at[slot],
            recv_sem=n2r_sem.at[slot],
            device_id={"sp": neighbour(half, 1, direction)},
            device_id_type=MESH,
        )

    for across in (2, 1, 3, 0):
        for half in range(2):
            red_s[half * RING + across] = total_of(half, across)
            if across == 2:
                far2_copy(half, 0).start()
                far2_copy(half, 1).start()
            elif across == 1:
                near2_copy(half, 1, 1).start()
            elif across == 3:
                near2_copy(half, -1, 0).start()
    for half in range(2):
        for direction, which in ((1, 0), (-1, 1)):
            far2_copy(half, which).wait_recv()
            at = half * RING + (1 if direction == 1 else 3)
            span = slice(which * quarter, (which + 1) * quarter)
            red_s[at, span, :] = red_s[at, span, :] + far2_r[half * 2 + which]
            near2_copy(half, direction, which).start()

    squares = jnp.zeros((1, cols), F32)
    for half in range(2):
        for which in range(2):
            for direction in (1, -1):
                near2_copy(half, direction, which).wait_recv()
            plus, minus = (half * 2) * 2 + which, (half * 2 + 1) * 2 + which
            span = slice(which * quarter, (which + 1) * quarter)
            done = red_s[half * RING, span, :] + near2_r[plus] + near2_r[minus]
            red_s[half * RING, span, :] = done
            squares = squares + jnp.sum(done * done, axis=0, keepdims=True)

    def norm_copy(source, target):
        return pltpu.make_async_remote_copy(
            src_ref=nmsg,
            dst_ref=nslots.at[source],
            send_sem=norm_s.at[target],
            recv_sem=norm_r.at[source],
            device_id={"tp": target},
            device_id_type=MESH,
        )

    nmsg[...] = jnp.broadcast_to(squares, (8, cols))
    for off in range(1, tp_count):
        norm_copy(my_tp, lax.rem(my_tp + off, tp_count)).start()
    for half in range(2):
        wg_ref[:, half * HEAD : (half + 1) * HEAD] = red_s[half * RING].T
    norms = squares
    for off in range(1, tp_count):
        source = lax.rem(my_tp + off, tp_count)
        norm_copy(source, my_tp).wait_recv()
        norms = norms + nslots[source, 0:1, :]
    rn_ref[...] = norms

    for off in range(1, RING):
        row_copy(grow, gs_sem, gr_sem, mx, lax.rem(mx + off, RING)).wait_send()
        row_copy(srow, ss_sem, sr_sem, mx, lax.rem(mx + off, RING)).wait_send()
    for target in range(RING):

        @pl.when(target < mz)
        def _(target=target):
            col_copy(gcol, gs2_sem, gr2_sem, mz, target).wait_send()

        @pl.when(target > mz)
        def _(target=target):
            col_copy(scol, ss2_sem, sr2_sem, mz, target).wait_send()

    for half in range(2):
        for across in range(RING):
            far_copy(half, across).wait_send()
            for direction in (1, -1):
                near_copy(half, direction, across).wait_send()
        for which in range(2):
            far2_copy(half, which).wait_send()
            for direction in (1, -1):
                near2_copy(half, direction, which).wait_send()
    for off in range(1, tp_count):
        norm_copy(my_tp, lax.rem(my_tp + off, tp_count)).wait_send()


def put_out(*refs):
    sources, targets, sems = refs[:6], refs[6:12], refs[12]
    copies = [pltpu.make_async_copy(s, t, sems.at[i]) for i, (s, t) in enumerate(zip(sources, targets))]
    for copy in copies:
        copy.start()
    for copy in copies:
        copy.wait()


def shards(sp_count, tp_count, block_input, value_weight, key_rows, query_rows, decay_pre, decay_log, gate_rows, out_grad):
    tokens, width = block_input.shape
    blocks = tokens // BLK
    lanes = 2 * HEAD
    cols = width // sp_count
    vmem = lambda shape, dtype=F32: pltpu.VMEM(shape, dtype)
    dma = lambda *shape: pltpu.SemaphoreType.DMA(shape)
    state_msg = (STATE + 8, lanes)
    scratch = [
        vmem((tokens, width), BF16), vmem((width, lanes), BF16), vmem((STATE, tokens), BF16), vmem((STATE, tokens), BF16),
        vmem((2, tokens)), pltpu.SMEM((2,), F32), vmem((tokens, lanes), BF16), vmem((tokens, lanes), BF16),
        vmem((2 * blocks, BLK)), vmem((BLK, BLK)), vmem((blocks, lanes)),
        vmem((tokens, lanes)), vmem((tokens, 2 * BLK)), vmem((tokens, 2 * BLK)), vmem((tokens, lanes)),
        vmem((tokens, lanes)), vmem((tokens, lanes)), vmem((tokens, lanes)), vmem((tokens, lanes)), vmem((tokens, lanes)),
        vmem((blocks + 1, STATE, lanes)), vmem((blocks, STATE, lanes)), vmem((blocks, STATE, lanes)),
        vmem((STATE, lanes)), vmem((STATE, lanes)), vmem((lanes, tokens), BF16),
        vmem((BLK, lanes)), vmem((BLK, lanes)), vmem((blocks, lanes)),
        vmem((STATE, lanes)), *(vmem((RING, *state_msg)) for _ in range(4)),
        vmem((sp_count, lanes, cols)), vmem((8, HEAD, cols)), vmem((16, HEAD, cols)), vmem((8, HEAD, cols)),
        vmem((4, HEAD // 2, cols)), vmem((8, HEAD // 2, cols)),
        vmem((8, cols)), vmem((tp_count, 8, cols)),
        dma(7), dma(max(2, tokens // (4 * BLK))), *(dma(RING) for _ in range(8)),
        dma(8), dma(8), dma(16), dma(16), dma(4), dma(4), dma(8), dma(8), dma(tp_count), dma(tp_count),
    ]
    hbm = pl.BlockSpec(memory_space=pltpu.HBM)
    in_vmem = pl.BlockSpec(memory_space=pltpu.VMEM)
    outs = pl.pallas_call(
        functools.partial(mixer, sp_count, tp_count),
        out_shape=(
            jax.ShapeDtypeStruct((STATE, tokens), F32),
            jax.ShapeDtypeStruct((STATE, tokens), F32),
            jax.ShapeDtypeStruct((2, tokens), F32),
            jax.ShapeDtypeStruct((tokens, lanes), F32),
            jax.ShapeDtypeStruct((cols, lanes), F32),
            jax.ShapeDtypeStruct((1, cols), F32),
        ),
        in_specs=[hbm] * 8,
        out_specs=tuple([in_vmem] * 6),
        scratch_shapes=scratch,
        compiler_params=pltpu.CompilerParams(
            collective_id=0, has_side_effects=True, vmem_limit_bytes=46 * 1024 * 1024
        ),
        name="mixer",
    )(
        *(pltpu.with_memory_space_constraint(a, pltpu.HBM) for a in (block_input, value_weight, key_rows.T, query_rows.T, decay_pre)),
        pltpu.with_memory_space_constraint(decay_log, pltpu.HBM),
        *(pltpu.with_memory_space_constraint(a, pltpu.HBM) for a in (gate_rows, out_grad)),
    )
    kg, qg, dg, gg, wg, rn = pl.pallas_call(
        put_out,
        out_shape=tuple(jax.ShapeDtypeStruct(o.shape, o.dtype) for o in outs),
        in_specs=[in_vmem] * 6,
        out_specs=tuple([hbm] * 6),
        scratch_shapes=[dma(6)],
        compiler_params=pltpu.CompilerParams(vmem_limit_bytes=8 * 1024 * 1024),
        name="put_out",
    )(*outs)
    return kg.T, qg.T, dg, gg, wg, rn.reshape(cols)


def solution(mesh):
    in_specs = (
        P("sp", None),
        P(None, "tp"),
        P("sp", "tp"),
        P("sp", "tp"),
        P("tp", "sp"),
        P("tp"),
        P("sp", "tp"),
        P("sp", "tp"),
    )
    out_specs = (P("sp", "tp"), P("sp", "tp"), P("tp", "sp"), P("sp", "tp"), P("sp", "tp"), P("sp"))
    body = functools.partial(shards, mesh.shape["sp"], mesh.shape["tp"])
    return jax.shard_map(body, mesh=mesh, in_specs=in_specs, out_specs=out_specs, check_vma=False)
```

```python
import functools

import jax
import jax.numpy as jnp
from jax import lax
from jax.experimental import pallas as pl
from jax.experimental.pallas import tpu as pltpu
from jax.sharding import PartitionSpec as P

HEAD = 64
STATE = 64
BLK = 128
RING = 4
F32 = jnp.float32
BF16 = jnp.bfloat16
HIGHEST = lax.Precision.HIGHEST
MESH = pl.DeviceIdType.MESH

ORDER = [
    [(2, 2)], [(2, 0), (0, 2)], [(2, 1), (1, 2)], [(2, 3), (3, 2)], [(1, 3), (3, 1)],
    [(3, 3), (1, 1)], [(1, 0), (0, 1)], [(3, 0), (0, 3)], [(0, 0)],
]


def nn(a, b, precision=None):
    return lax.dot_general(a, b, (((1,), (0,)), ((), ())), precision=precision, preferred_element_type=F32)


def nt(a, b, precision=None):
    return lax.dot_general(a, b, (((1,), (1,)), ((), ())), precision=precision, preferred_element_type=F32)


def tn(a, b, precision=None):
    return lax.dot_general(a, b, (((0,), (0,)), ((), ())), precision=precision, preferred_element_type=F32)


def halves(a):
    high = a.astype(BF16)
    return high, (a - high.astype(F32)).astype(BF16)


def both(a):
    return jnp.concatenate(halves(a), axis=1)


def folded(a):
    width = a.shape[1] // 2
    return a[:, :width] + a[:, width:]


def softplus(a):
    return jnp.maximum(a, 0.0) + jnp.log1p(jnp.exp(-jnp.abs(a)))


def sigmoid(a):
    return 1.0 / (1.0 + jnp.exp(-a))


def mixer(
    sp_count,
    tp_count,
    x_hbm, w_hbm, k_hbm, q_hbm, pre_hbm, rate_hbm, gate_hbm, cot_hbm,
    kg_ref, qg_ref, dg_ref, gg_ref, wg_ref, rn_ref,
    m_s,
    x_v, w_v, k_v, q_v, pre_v, rate_ref, gate_v, cot_v,
    rows_s, stack_s, rend_s,
    dy_s, tm_s, lm_s, er_s, te_s, se_s, p_s, v_s, u_s,
    gst_s, sst_s, bs_s, out_s, inc_s, vgt_s,
    yy_s, dd_s, ee_s,
    last_s, grow, gcol, srow, scol,
    part, far_r, near_r, red_s, far2_r, near2_r,
    nmsg, nslots,
    in_sem, x_sem, gs_sem, gr_sem, ss_sem, sr_sem, gs2_sem, gr2_sem, ss2_sem, sr2_sem,
    fs_sem, fr_sem, ns_sem, nr_sem, f2s_sem, f2r_sem, n2s_sem, n2r_sem, norm_s, norm_r,
):
    tokens, width = x_v.shape
    blocks = tokens // BLK
    lanes = 2 * HEAD
    cols = width // sp_count
    me = lax.axis_index("sp")
    my_tp = lax.axis_index("tp")
    mz, mx = lax.div(me, RING), lax.rem(me, RING)

    barrier = pltpu.get_barrier_semaphore()
    for off in range(1, RING):
        for peer in (mz * RING + lax.rem(mx + off, RING), lax.rem(mz + off, RING) * RING + mx):
            pl.semaphore_signal(barrier, inc=1, device_id={"sp": peer}, device_id_type=MESH)
    for off in range(1, tp_count):
        pl.semaphore_signal(
            barrier, inc=1, device_id={"tp": lax.rem(my_tp + off, tp_count)}, device_id_type=MESH
        )

    small = [
        pltpu.make_async_copy(src, dst, in_sem.at[i])
        for i, (src, dst) in enumerate(
            [
                (pre_hbm, pre_v), (rate_hbm, rate_ref), (gate_hbm, gate_v), (cot_hbm, cot_v), (q_hbm, q_v), (k_hbm, k_v), (w_hbm, w_v)
            ]
        )
    ]
    for copy in small[:6]:
        copy.start()
    xrows = tokens // x_sem.shape[0]
    xchunks = tokens // xrows

    def x_copy(i):
        rows = pl.ds(pl.multiple_of(i * xrows, xrows), xrows)
        return pltpu.make_async_copy(x_hbm.at[rows], x_v.at[rows], x_sem.at[i])

    small[0].wait()
    small[1].wait()
    for h in range(2):
        for c in range(blocks):
            rows_s[h * blocks + c : h * blocks + c + 1, :] = pre_v[h : h + 1, c * BLK : (c + 1) * BLK]
    pre = rows_s[...]
    row_id = lax.broadcasted_iota(jnp.int32, (2 * blocks, BLK), 0)
    rate = jnp.where(
        row_id < blocks,
        jnp.exp(jnp.full((2 * blocks, BLK), rate_ref[0], F32)),
        jnp.exp(jnp.full((2 * blocks, BLK), rate_ref[1], F32)),
    )
    step = softplus(pre)
    sq_row = lax.broadcasted_iota(jnp.int32, (BLK, BLK), 0)
    sq_col = lax.broadcasted_iota(jnp.int32, (BLK, BLK), 1)
    upper = sq_row <= sq_col
    lower = sq_row >= sq_col
    run = nn(-rate * step, (sq_row <= sq_col).astype(F32), HIGHEST)
    stack_s[...] = jnp.zeros_like(stack_s)
    stack_s[0 : 2 * blocks, :] = run
    stack_s[2 * blocks : 4 * blocks, :] = step
    turned = stack_s[...].T
    first_head = lax.broadcasted_iota(jnp.int32, (BLK, lanes), 1) < HEAD
    for copy in small[2:6]:
        copy.wait()
    small[6].start()
    for i in range(xchunks):
        x_copy(i).start()

    def block_rows(c):
        return pl.ds(pl.multiple_of(c * BLK, BLK), BLK)

    def for_blocks(start, stop, unroll, body):
        def step_of(i, carry):
            for b in range(unroll):
                body(start + i * unroll + b)
            return carry

        lax.fori_loop(0, (stop - start) // unroll, step_of, 0)

    def columns_of(c, kinds):
        rolled = pltpu.roll(turned, lax.rem(BLK - c, BLK), 1)
        return [jnp.broadcast_to(rolled[:, i * blocks : i * blocks + 1], (BLK, BLK)) for i in kinds]

    def prepare(c):
        rows = block_rows(c)
        running = jnp.where(first_head, *columns_of(c, (0, 1)))
        er = jnp.exp(running)
        er_s[rows, :] = er
        rend_s[pl.ds(c, 1), :] = running[BLK - 1 : BLK, :]
        gate = gate_v[rows, :].astype(F32)
        dy = cot_v[rows, :].astype(F32) * gate * sigmoid(gate)
        dy_s[rows, :] = dy
        bs_s[c] = folded(nn(q_v[:, rows], both(er * dy)))

    for_blocks(0, blocks, min(8, blocks), prepare)
    grad = jnp.zeros((STATE, lanes), F32)
    total = jnp.zeros((1, lanes), F32)
    for c in reversed(range(blocks)):
        end = rend_s[c : c + 1, :]
        grad = jnp.exp(end) * grad + bs_s[c]
        total = total + end
        gst_s[c] = grad
    def message(ref, at, value, log):
        ref[at, 0:STATE, :] = value
        ref[at, STATE : STATE + 8, :] = jnp.broadcast_to(log, (8, lanes))

    def row_copy(slots, send, recv, target):
        return pltpu.make_async_remote_copy(
            src_ref=slots.at[mx],
            dst_ref=slots.at[mx],
            send_sem=send.at[0],
            recv_sem=recv.at[0],
            device_id={"sp": mz * RING + target},
            device_id_type=MESH,
        )

    def all_of(refs, send, recv):
        return pltpu.make_async_remote_copy(
            src_ref=refs,
            dst_ref=refs,
            send_sem=send,
            recv_sem=recv,
            device_id={"sp": mz * RING + lax.rem(mx + 1, RING)},
            device_id_type=MESH,
        )

    def col_copy(slots, send, recv, source, target):
        return pltpu.make_async_remote_copy(
            src_ref=slots.at[source],
            dst_ref=slots.at[source],
            send_sem=send.at[target],
            recv_sem=recv.at[source],
            device_id={"sp": target * RING + mx},
            device_id_type=MESH,
        )

    def send_row(slots, send, recv):
        for off in (2, 1, 3):
            row_copy(slots, send, recv, lax.rem(mx + off, RING)).start()

    def row_sum(slots, send, recv, order):
        all_of(slots.at[0 : RING - 1], send.at[0], recv.at[0]).wait_recv()
        acc = jnp.zeros((STATE, lanes), F32)
        log = jnp.zeros((1, lanes), F32)
        own, own_log = acc, log
        for at in order:
            own = jnp.where(mx == at, acc, own)
            own_log = jnp.where(mx == at, log, own_log)
            tail = slots[at, STATE : STATE + 1, :]
            acc = slots[at, 0:STATE, :] + jnp.exp(tail) * acc
            log = log + tail
        return own, own_log, acc, log

    message(grow, mx, grad, total)
    pl.semaphore_wait(barrier, 2 * (RING - 1) + tp_count - 1)
    send_row(grow, gs_sem, gr_sem)

    def project(i):
        x_copy(i).wait()
        rows = pl.ds(pl.multiple_of(i * xrows, xrows), xrows)
        p_s[rows, :] = nn(x_v[rows, :], w_v[...]).astype(BF16).astype(F32)

    def local(c):
        rows = block_rows(c)
        col = columns_of(c, range(4))
        pair = pl.ds(pl.multiple_of(c * 2 * BLK, 2 * BLK), 2 * BLK)
        scores = tn(k_v[:, rows], q_v[:, rows])
        decay = jnp.concatenate(
            [
                jnp.exp(jnp.where(upper, stack_s[pl.ds(h * blocks + c, 1), :] - col[h], -1e30))
                for h in range(2)
            ],
            axis=0,
        )
        lm_s[pair, :] = decay
        running = jnp.where(first_head, col[0], col[1])
        te_s[rows, :] = jnp.exp(running[BLK - 1 : BLK, :] - running)
        se_s[rows, :] = jnp.where(first_head, col[2], col[3])
        dy_high, dy_low = halves(dy_s[rows, :])
        t_high, t_low = halves(jnp.concatenate([scores, scores], axis=0) * decay)
        tm_s[pair, :] = t_high
        u = folded(nn(t_high, jnp.concatenate([dy_high, dy_low], axis=1))) + nn(t_low, dy_high)
        u_s[rows, :] = jnp.where(first_head, u[0:BLK, :], u[BLK : 2 * BLK, :])

    def with_values(c):
        rows = block_rows(c)
        projected = p_s[rows, :]
        v = projected * sigmoid(projected)
        v_s[rows, :] = v
        bs_s[c] = folded(nn(k_v[:, rows], both(te_s[rows, :] * se_s[rows, :] * v)))

    for_blocks(0, blocks, min(4, blocks), local)
    small[6].wait()

    def chunk(i, carry):
        project(i)
        return carry

    own_grad, own_log, ring_grad, ring_log = row_sum(grow, gs_sem, gr_sem, (3, 2, 1, 0))
    message(gcol, mz, ring_grad, ring_log)
    for target in (1, 0, 2):

        @pl.when(target < mz)
        def _(target=target):
            col_copy(gcol, gs2_sem, gr2_sem, mz, target).start()

    lax.fori_loop(0, xchunks, chunk, 0)
    for_blocks(0, blocks, min(4, blocks), with_values)
    state = jnp.zeros((STATE, lanes), F32)
    for c in range(blocks):
        sst_s[c] = state
        state = jnp.exp(rend_s[c : c + 1, :]) * state + bs_s[c]
    last_s[...] = state
    message(srow, mx, state, total)
    send_row(srow, ss_sem, sr_sem)

    out_s[...] = jnp.zeros_like(out_s)
    for source in reversed(range(1, RING)):

        @pl.when(source > mz)
        def _(source=source):
            col_copy(gcol, gs2_sem, gr2_sem, source, mz).wait_recv()
            out_s[...] = gcol[source, 0:STATE, :] + jnp.exp(gcol[source, STATE : STATE + 1, :]) * out_s[...]

    out_s[...] = own_grad + jnp.exp(own_log) * out_s[...]
    after = jnp.zeros((1, lanes), F32)
    for c in reversed(range(blocks)):
        after = after + rend_s[c : c + 1, :]
        gst_s[c] = gst_s[c] + jnp.exp(after) * out_s[...]
    gst_s[blocks] = out_s[...]

    def value_gradient(c):
        rows = block_rows(c)
        u = u_s[rows, :] + te_s[rows, :] * folded(tn(k_v[:, rows], both(gst_s[c + 1])))
        u_s[rows, :] = u
        projected = p_s[rows, :]
        sig = sigmoid(projected)
        vg = se_s[rows, :] * u * sig * (1.0 + projected * (1.0 - sig))
        vgt_s[:, rows] = vg.astype(BF16).T

    for_blocks(0, blocks, min(4, blocks), value_gradient)

    def owner(dz, dx):
        return lax.rem(mz + dz, RING) * RING + lax.rem(mx + dx, RING)

    def neighbour(half, stage, direction):
        if half == stage:
            return lax.rem(mz + direction + RING, RING) * RING + mx
        return mz * RING + lax.rem(mx + direction + RING, RING)

    def half_of(half, dz, dx):
        return part.at[owner(dz, dx), half * HEAD : (half + 1) * HEAD, :]

    def piece(half, dist, across):
        return half_of(half, dist, across) if half == 0 else half_of(half, across, dist)

    def far_copy(half, across):
        direction = 1 if across < 2 else -1
        slot = half * RING + across
        return pltpu.make_async_remote_copy(
            src_ref=piece(half, 2, across),
            dst_ref=far_r.at[slot],
            send_sem=fs_sem.at[0],
            recv_sem=fr_sem.at[slot],
            device_id={"sp": neighbour(half, 0, direction)},
            device_id_type=MESH,
        )

    def near_copy(half, direction, across):
        pair = half * RING + across
        return pltpu.make_async_remote_copy(
            src_ref=piece(half, 1 if direction == 1 else 3, across),
            dst_ref=near_r.at[2 * pair + (0 if direction == 1 else 1)],
            send_sem=ns_sem.at[0],
            recv_sem=nr_sem.at[pair],
            device_id={"sp": neighbour(half, 0, direction)},
            device_id_type=MESH,
        )

    for group in ORDER:
        for dz, dx in group:
            dest = owner(dz, dx)
            columns = pl.ds(pl.multiple_of(dest * cols, cols), cols)
            part[dest] = nn(vgt_s[...], x_v[:, columns])
        for dz, dx in group:
            for half, dist, across in ((0, dz, dx), (1, dx, dz)):
                if dist == 2:
                    far_copy(half, across).start()
                elif dist == 1 and across >= 2:
                    near_copy(half, 1, across).start()
                elif dist == 3 and across < 2:
                    near_copy(half, -1, across).start()
    zero = jnp.zeros((BLK, lanes), BF16)
    lane_id = lax.broadcasted_iota(jnp.int32, (BLK, lanes), 1)
    yy_s[...] = jnp.zeros_like(yy_s)
    dd_s[...] = jnp.zeros_like(dd_s)

    def keep_head_sums(ref, c, a):
        first = jnp.sum(jnp.where(first_head, a, 0.0), axis=1, keepdims=True)
        second = jnp.sum(jnp.where(first_head, 0.0, a), axis=1, keepdims=True)
        ref[...] = jnp.where(lane_id == c, first, jnp.where(lane_id == blocks + c, second, ref[...]))

    def split_heads(a):
        return jnp.concatenate([jnp.where(first_head, a, zero), jnp.where(first_head, zero, a)], axis=0)

    def span_only(c):
        rows = block_rows(c)
        pair = pl.ds(pl.multiple_of(c * 2 * BLK, 2 * BLK), 2 * BLK)
        q, k = q_v[:, rows], k_v[:, rows]
        v = v_s[rows, :]
        sv = se_s[rows, :] * v
        sv_high, sv_low = halves(sv)
        by_head = split_heads(sv_high)
        m_s[rows, :] = folded(tn(tm_s[pair, :], jnp.concatenate([by_head, split_heads(sv_low)], axis=1)))
        d = nt(by_head, dy_s[rows, :].astype(BF16)) * lm_s[pair, :]
        d_high, d_low = halves(d[0:BLK, :] + d[BLK : 2 * BLK, :])
        kg_ref[:, rows] = nt(
            jnp.concatenate([q, q], axis=1), jnp.concatenate([d_high, d_low], axis=1)
        ) + nt(gst_s[c + 1].astype(BF16), (te_s[rows, :] * sv).astype(BF16))
        qg_ref[:, rows] = nn(jnp.concatenate([k, k], axis=1), jnp.concatenate([d_high, d_low], axis=0))
        keep_head_sums(dd_s, c, v * u_s[rows, :])

    def with_entering(c):
        rows = block_rows(c)
        dy, er = dy_s[rows, :], er_s[rows, :]
        mixed = m_s[rows, :] + er * folded(tn(q_v[:, rows], both(sst_s[c])))
        gate = gate_v[rows, :].astype(F32)
        sig = sigmoid(gate)
        gg_ref[rows, :] = cot_v[rows, :].astype(F32) * mixed * sig * (1.0 + gate * (1.0 - sig))
        qg_ref[:, rows] = qg_ref[:, rows] + nt(sst_s[c].astype(BF16), (er * dy).astype(BF16))
        keep_head_sums(yy_s, c, dy * mixed)

    steps = (4, blocks // 2, blocks * 3 // 4) if blocks >= 16 else (1, blocks // 2, blocks // 2)
    for_blocks(0, steps[1], steps[0], span_only)
    for direction, lane in ((-1, 2), (1, 0), (1, 1), (-1, 3)):
        for half in range(2):
            far_copy(half, lane).wait_recv()
            ref = piece(half, 1 if direction == 1 else 3, lane)
            ref[...] = ref[...] + far_r[half * RING + lane]
            near_copy(half, direction, lane).start()

    own_state, own_state_log, ring_state, ring_log = row_sum(srow, ss_sem, sr_sem, (0, 1, 2, 3))
    message(scol, mz, ring_state, ring_log)
    for target in range(1, RING):

        @pl.when(target > mz)
        def _(target=target):
            col_copy(scol, ss2_sem, sr2_sem, mz, target).start()

    for_blocks(steps[1], steps[2], steps[0], span_only)

    quarter = HEAD // 2

    def total_of(half, across):
        pair = half * RING + across
        all_of(near_r.at[2 * pair : 2 * pair + 2], ns_sem.at[0], nr_sem.at[pair]).wait_recv()
        return piece(half, 0, across)[...] + near_r[2 * pair] + near_r[2 * pair + 1]

    def far2_copy(half, which):
        slot = half * 2 + which
        return pltpu.make_async_remote_copy(
            src_ref=red_s.at[half * RING + 2, which * quarter : (which + 1) * quarter, :],
            dst_ref=far2_r.at[slot],
            send_sem=f2s_sem.at[0],
            recv_sem=f2r_sem.at[slot],
            device_id={"sp": neighbour(half, 1, 1 if which == 0 else -1)},
            device_id_type=MESH,
        )

    def near2_copy(half, direction, which):
        pair = half * 2 + which
        return pltpu.make_async_remote_copy(
            src_ref=red_s.at[half * RING + (1 if direction == 1 else 3), which * quarter : (which + 1) * quarter, :],
            dst_ref=near2_r.at[2 * pair + (0 if direction == 1 else 1)],
            send_sem=n2s_sem.at[0],
            recv_sem=n2r_sem.at[pair],
            device_id={"sp": neighbour(half, 1, direction)},
            device_id_type=MESH,
        )

    for across in (2, 1, 3, 0):
        if across == 1:
            for_blocks(steps[2], blocks, steps[0], span_only)
        for half in range(2):
            red_s[half * RING + across] = total_of(half, across)
            if across == 2:
                far2_copy(half, 0).start()
                far2_copy(half, 1).start()
            elif across == 1:
                near2_copy(half, 1, 1).start()
            elif across == 3:
                near2_copy(half, -1, 0).start()
    for half in range(2):
        for direction, which in ((1, 0), (-1, 1)):
            far2_copy(half, which).wait_recv()
            at = half * RING + (1 if direction == 1 else 3)
            span = slice(which * quarter, (which + 1) * quarter)
            red_s[at, span, :] = red_s[at, span, :] + far2_r[half * 2 + which]
            near2_copy(half, direction, which).start()

    inc_s[...] = jnp.zeros_like(inc_s)
    for source in range(RING - 1):

        @pl.when(source < mz)
        def _(source=source):
            col_copy(scol, ss2_sem, sr2_sem, source, mz).wait_recv()
            inc_s[...] = scol[source, 0:STATE, :] + jnp.exp(scol[source, STATE : STATE + 1, :]) * inc_s[...]

    inc_s[...] = own_state + jnp.exp(own_state_log) * inc_s[...]
    before = jnp.zeros((1, lanes), F32)
    for c in range(blocks):
        full = sst_s[c] + jnp.exp(before) * inc_s[...]
        sst_s[c] = full
        before = before + rend_s[c : c + 1, :]
        if c > 0:
            ee_s[c - 1 : c, :] = jnp.sum(full * gst_s[c], axis=0, keepdims=True)
    last = last_s[...] + jnp.exp(before) * inc_s[...]
    ee_s[blocks - 1 : blocks, :] = jnp.sum(last * gst_s[blocks], axis=0, keepdims=True)

    later = blocks * 3 // 4 if blocks >= 8 else blocks // 2
    for_blocks(0, later, min(4, later), with_entering)

    squares = jnp.zeros((1, cols), F32)
    for half in range(2):
        for which in range(2):
            pair = half * 2 + which
            all_of(near2_r.at[2 * pair : 2 * pair + 2], n2s_sem.at[0], n2r_sem.at[pair]).wait_recv()
            span = slice(which * quarter, (which + 1) * quarter)
            done = red_s[half * RING, span, :] + near2_r[2 * pair] + near2_r[2 * pair + 1]
            red_s[half * RING, span, :] = done
            squares = squares + jnp.sum(done * done, axis=0, keepdims=True)

    def norm_copy(source, target):
        return pltpu.make_async_remote_copy(
            src_ref=nmsg,
            dst_ref=nslots.at[source],
            send_sem=norm_s.at[0],
            recv_sem=norm_r.at[0],
            device_id={"tp": target},
            device_id_type=MESH,
        )

    nmsg[...] = jnp.broadcast_to(squares, (8, cols))
    for off in range(1, tp_count):
        norm_copy(my_tp, lax.rem(my_tp + off, tp_count)).start()
    for_blocks(later, blocks, min(4, blocks - later), with_entering)
    ends = ee_s[...]
    end_cols = jnp.concatenate(
        [
            jnp.sum(ends[:, 0:HEAD], axis=1, keepdims=True),
            jnp.sum(ends[:, HEAD:lanes], axis=1, keepdims=True),
        ],
        axis=0,
    )
    direct = dd_s[...].T[0 : 2 * blocks, :]
    log_grad = nn(yy_s[...].T[0 : 2 * blocks, :] - step * direct, lower.astype(F32), HIGHEST) + end_cols
    decay_grad = (direct - rate * log_grad) * sigmoid(pre)
    for h in range(2):
        for c in range(blocks):
            dg_ref[h : h + 1, c * BLK : (c + 1) * BLK] = decay_grad[h * blocks + c : h * blocks + c + 1, :]
    for half in range(2):
        wg_ref[:, half * HEAD : (half + 1) * HEAD] = red_s[half * RING].T
    norms = squares
    if tp_count > 1:
        all_of(nslots.at[0 : tp_count - 1], norm_s.at[0], norm_r.at[0]).wait_recv()
    for off in range(1, tp_count):
        norms = norms + nslots[lax.rem(my_tp + off, tp_count), 0:1, :]
    rn_ref[...] = norms

    all_of(grow.at[0 : RING - 1], gs_sem.at[0], gr_sem.at[0]).wait_send()
    all_of(srow.at[0 : RING - 1], ss_sem.at[0], sr_sem.at[0]).wait_send()
    for target in range(RING):

        @pl.when(target < mz)
        def _(target=target):
            col_copy(gcol, gs2_sem, gr2_sem, mz, target).wait_send()

        @pl.when(target > mz)
        def _(target=target):
            col_copy(scol, ss2_sem, sr2_sem, mz, target).wait_send()

    all_of(far_r, fs_sem.at[0], fr_sem.at[0]).wait_send()
    all_of(near_r, ns_sem.at[0], nr_sem.at[0]).wait_send()
    all_of(far2_r, f2s_sem.at[0], f2r_sem.at[0]).wait_send()
    all_of(near2_r, n2s_sem.at[0], n2r_sem.at[0]).wait_send()
    if tp_count > 1:
        all_of(nslots.at[0 : tp_count - 1], norm_s.at[0], norm_r.at[0]).wait_send()


def put_out(*refs):
    sources, targets, sems = refs[:6], refs[6:12], refs[12]
    copies = [pltpu.make_async_copy(s, t, sems.at[i]) for i, (s, t) in enumerate(zip(sources, targets))]
    for copy in copies:
        copy.start()
    for copy in copies:
        copy.wait()


def shards(sp_count, tp_count, block_input, value_weight, key_rows, query_rows, decay_pre, decay_log, gate_rows, out_grad):
    tokens, width = block_input.shape
    blocks = tokens // BLK
    lanes = 2 * HEAD
    cols = width // sp_count
    vmem = lambda shape, dtype=F32: pltpu.VMEM(shape, dtype)
    dma = lambda *shape: pltpu.SemaphoreType.DMA(shape)
    state_msg = (STATE + 8, lanes)
    scratch = [
        vmem((tokens, lanes)),
        vmem((tokens, width), BF16), vmem((width, lanes), BF16), vmem((STATE, tokens), BF16), vmem((STATE, tokens), BF16),
        vmem((2, tokens)), pltpu.SMEM((2,), F32), vmem((tokens, lanes), BF16), vmem((tokens, lanes), BF16),
        vmem((2 * blocks, BLK)), vmem((BLK, BLK)), vmem((blocks, lanes)),
        vmem((tokens, lanes)), vmem((2 * tokens, BLK), BF16), vmem((2 * tokens, BLK)), vmem((tokens, lanes)),
        vmem((tokens, lanes)), vmem((tokens, lanes)), vmem((tokens, lanes)), vmem((tokens, lanes)), vmem((tokens, lanes)),
        vmem((blocks + 1, STATE, lanes)), vmem((blocks, STATE, lanes)), vmem((blocks, STATE, lanes)),
        vmem((STATE, lanes)), vmem((STATE, lanes)), vmem((lanes, tokens), BF16),
        vmem((BLK, lanes)), vmem((BLK, lanes)), vmem((blocks, lanes)),
        vmem((STATE, lanes)), *(vmem((RING, *state_msg)) for _ in range(4)),
        vmem((sp_count, lanes, cols)), vmem((8, HEAD, cols)), vmem((16, HEAD, cols)), vmem((8, HEAD, cols)),
        vmem((4, HEAD // 2, cols)), vmem((8, HEAD // 2, cols)),
        vmem((8, cols)), vmem((tp_count, 8, cols)),
        dma(7), dma(max(2, tokens // (4 * BLK))), *(dma(1) for _ in range(4)), *(dma(RING) for _ in range(4)),
        dma(1), dma(8), dma(1), dma(8), dma(1), dma(4), dma(1), dma(4), dma(1), dma(1),
    ]
    hbm = pl.BlockSpec(memory_space=pltpu.HBM)
    in_vmem = pl.BlockSpec(memory_space=pltpu.VMEM)
    outs = pl.pallas_call(
        functools.partial(mixer, sp_count, tp_count),
        out_shape=(
            jax.ShapeDtypeStruct((STATE, tokens), F32),
            jax.ShapeDtypeStruct((STATE, tokens), F32),
            jax.ShapeDtypeStruct((2, tokens), F32),
            jax.ShapeDtypeStruct((tokens, lanes), F32),
            jax.ShapeDtypeStruct((cols, lanes), F32),
            jax.ShapeDtypeStruct((1, cols), F32),
        ),
        in_specs=[hbm] * 8,
        out_specs=tuple([in_vmem] * 6),
        scratch_shapes=scratch,
        compiler_params=pltpu.CompilerParams(
            collective_id=0, has_side_effects=True, vmem_limit_bytes=46 * 1024 * 1024
        ),
        name="mixer",
    )(
        *(pltpu.with_memory_space_constraint(a, pltpu.HBM) for a in (block_input, value_weight, key_rows.T, query_rows.T, decay_pre)),
        pltpu.with_memory_space_constraint(decay_log, pltpu.HBM),
        *(pltpu.with_memory_space_constraint(a, pltpu.HBM) for a in (gate_rows, out_grad)),
    )
    kg, qg, dg, gg, wg, rn = pl.pallas_call(
        put_out,
        out_shape=tuple(jax.ShapeDtypeStruct(o.shape, o.dtype) for o in outs),
        in_specs=[in_vmem] * 6,
        out_specs=tuple([hbm] * 6),
        scratch_shapes=[dma(6)],
        compiler_params=pltpu.CompilerParams(vmem_limit_bytes=8 * 1024 * 1024),
        name="put_out",
    )(*outs)
    return kg.T, qg.T, dg, gg, wg, rn.reshape(cols)


def solution(mesh):
    in_specs = (
        P("sp", None),
        P(None, "tp"),
        P("sp", "tp"),
        P("sp", "tp"),
        P("tp", "sp"),
        P("tp"),
        P("sp", "tp"),
        P("sp", "tp"),
    )
    out_specs = (P("sp", "tp"), P("sp", "tp"), P("tp", "sp"), P("sp", "tp"), P("sp", "tp"), P("sp"))
    body = functools.partial(shards, mesh.shape["sp"], mesh.shape["tp"])
    return jax.shard_map(body, mesh=mesh, in_specs=in_specs, out_specs=out_specs, check_vma=False)
```

```python
import functools

import jax
import jax.numpy as jnp
from jax import lax
from jax.experimental import pallas as pl
from jax.experimental.pallas import tpu as pltpu
from jax.sharding import PartitionSpec as P

HEAD = 64
STATE = 64
BLK = 128
RING = 4
F32 = jnp.float32
BF16 = jnp.bfloat16
HIGHEST = lax.Precision.HIGHEST
MESH = pl.DeviceIdType.MESH

ORDER = [
    [(2, 2)], [(2, 0), (0, 2)], [(2, 1), (1, 2)], [(2, 3), (3, 2)], [(1, 3), (3, 1)],
    [(3, 3), (1, 1)], [(1, 0), (0, 1)], [(3, 0), (0, 3)], [(0, 0)],
]


def nn(a, b, precision=None):
    return lax.dot_general(a, b, (((1,), (0,)), ((), ())), precision=precision, preferred_element_type=F32)


def nt(a, b, precision=None):
    return lax.dot_general(a, b, (((1,), (1,)), ((), ())), precision=precision, preferred_element_type=F32)


def tn(a, b, precision=None):
    return lax.dot_general(a, b, (((0,), (0,)), ((), ())), precision=precision, preferred_element_type=F32)


def halves(a):
    high = a.astype(BF16)
    return high, (a - high.astype(F32)).astype(BF16)


def both(a):
    return jnp.concatenate(halves(a), axis=1)


def folded(a):
    width = a.shape[1] // 2
    return a[:, :width] + a[:, width:]


def softplus(a):
    return jnp.maximum(a, 0.0) + jnp.log1p(jnp.exp(-jnp.abs(a)))


def sigmoid(a):
    return 1.0 / (1.0 + jnp.exp(-a))


def mixer(
    sp_count,
    tp_count,
    x_hbm, w_hbm, k_hbm, q_hbm, pre_hbm, rate_hbm, gate_hbm, cot_hbm,
    kg_ref, qg_ref, dg_ref, gg_ref, wg_ref, rn_ref,
    m_s,
    x_v, w_v, k_v, q_v, pre_v, rate_ref, gate_v, cot_v,
    rows_s, stack_s, rend_s, fend_s,
    dy_s, tm_s, lm_s, er_s, te_s, se_s, p_s, v_s, u_s,
    gst_s, sst_s, bs_s, out_s, inc_s, vgt_s,
    yy_s, dd_s, ee_s,
    last_s, grow, gcol, srow, scol,
    part, far_r, near_r, red_s, second_r,
    nmsg, nslots,
    in_sem, x_sem, gs_sem, gr_sem, ss_sem, sr_sem, gs2_sem, gr2_sem, ss2_sem, sr2_sem,
    far_s, far_sem, near_s, near_sem, second_s, second_sem, norm_s, norm_r,
):
    tokens, width = x_v.shape
    blocks = tokens // BLK
    lanes = 2 * HEAD
    cols = width // sp_count
    me = lax.axis_index("sp")
    my_tp = lax.axis_index("tp")
    mz, mx = lax.div(me, RING), lax.rem(me, RING)

    barrier = pltpu.get_barrier_semaphore()
    for off in range(1, RING):
        for peer in (mz * RING + lax.rem(mx + off, RING), lax.rem(mz + off, RING) * RING + mx):
            pl.semaphore_signal(barrier, inc=1, device_id={"sp": peer}, device_id_type=MESH)
    for off in range(1, tp_count):
        pl.semaphore_signal(
            barrier, inc=1, device_id={"tp": lax.rem(my_tp + off, tp_count)}, device_id_type=MESH
        )

    small = [
        pltpu.make_async_copy(src, dst, in_sem.at[i])
        for i, (src, dst) in enumerate(
            [
                (pre_hbm, pre_v), (rate_hbm, rate_ref), (gate_hbm, gate_v), (cot_hbm, cot_v), (q_hbm, q_v), (k_hbm, k_v), (w_hbm, w_v)
            ]
        )
    ]
    for copy in small[:6]:
        copy.start()
    xrows = tokens // x_sem.shape[0]
    xchunks = tokens // xrows

    def x_copy(i):
        rows = pl.ds(pl.multiple_of(i * xrows, xrows), xrows)
        return pltpu.make_async_copy(x_hbm.at[rows], x_v.at[rows], x_sem.at[i])

    small[0].wait()
    small[1].wait()
    for h in range(2):
        for c in range(blocks):
            rows_s[h * blocks + c : h * blocks + c + 1, :] = pre_v[h : h + 1, c * BLK : (c + 1) * BLK]
    pre = rows_s[...]
    row_id = lax.broadcasted_iota(jnp.int32, (2 * blocks, BLK), 0)
    rate = jnp.where(
        row_id < blocks,
        jnp.exp(jnp.full((2 * blocks, BLK), rate_ref[0], F32)),
        jnp.exp(jnp.full((2 * blocks, BLK), rate_ref[1], F32)),
    )
    step = softplus(pre)
    sq_row = lax.broadcasted_iota(jnp.int32, (BLK, BLK), 0)
    sq_col = lax.broadcasted_iota(jnp.int32, (BLK, BLK), 1)
    upper = sq_row <= sq_col
    lower = sq_row >= sq_col
    run = nn(-rate * step, (sq_row <= sq_col).astype(F32), HIGHEST)
    if 8 * blocks < BLK:
        stack_s[...] = jnp.zeros_like(stack_s)
    stack_s[0 : 2 * blocks, :] = run
    stack_s[2 * blocks : 4 * blocks, :] = step
    stack_s[4 * blocks : 6 * blocks, :] = jnp.exp(run)
    stack_s[6 * blocks : 8 * blocks, :] = jnp.exp(run[:, BLK - 1 : BLK] - run)
    turned = stack_s[...].T
    rend = jnp.where(
        lax.broadcasted_iota(jnp.int32, (blocks, lanes), 1) < HEAD,
        run[0:blocks, BLK - 1 : BLK],
        run[blocks : 2 * blocks, BLK - 1 : BLK],
    )
    rend_s[...] = rend
    fend_s[...] = jnp.exp(rend)
    first_head = lax.broadcasted_iota(jnp.int32, (BLK, lanes), 1) < HEAD
    for copy in small[2:6]:
        copy.wait()
    small[6].start()
    x_copy(0).start()

    def block_rows(c):
        return pl.ds(c * BLK if isinstance(c, int) else pl.multiple_of(c * BLK, BLK), BLK)

    def for_blocks(start, stop, unroll, body):
        if unroll == stop - start:
            for c in range(start, stop):
                body(c)
            return

        def step_of(i, carry):
            for b in range(unroll):
                body(start + i * unroll + b)
            return carry

        lax.fori_loop(0, (stop - start) // unroll, step_of, 0)

    def columns_of(c, kinds):
        return [jnp.broadcast_to(turned[:, i * blocks + c : i * blocks + c + 1], (BLK, BLK)) for i in kinds]

    def prepare(c):
        rows = block_rows(c)
        er = jnp.where(first_head, *columns_of(c, (4, 5)))
        er_s[rows, :] = er
        gate = gate_v[rows, :].astype(F32)
        dy = cot_v[rows, :].astype(F32) * gate * sigmoid(gate)
        dy_s[rows, :] = dy
        bs_s[c] = folded(nn(q_v[:, rows], both(er * dy)))

    for_blocks(0, blocks, blocks, prepare)
    grad = jnp.zeros((STATE, lanes), F32)
    total = jnp.zeros((1, lanes), F32)
    for c in reversed(range(blocks)):
        end = rend_s[c : c + 1, :]
        grad = fend_s[c : c + 1, :] * grad + bs_s[c]
        total = total + end
        gst_s[c] = grad
    def message(ref, at, value, log):
        ref[at, 0:STATE, :] = value
        ref[at, STATE : STATE + 8, :] = jnp.broadcast_to(log, (8, lanes))

    def row_copy(slots, send, recv, target):
        return pltpu.make_async_remote_copy(
            src_ref=slots.at[mx],
            dst_ref=slots.at[mx],
            send_sem=send.at[0],
            recv_sem=recv.at[0],
            device_id={"sp": mz * RING + target},
            device_id_type=MESH,
        )

    def all_of(refs, send, recv):
        return pltpu.make_async_remote_copy(
            src_ref=refs,
            dst_ref=refs,
            send_sem=send,
            recv_sem=recv,
            device_id={"sp": mz * RING + lax.rem(mx + 1, RING)},
            device_id_type=MESH,
        )

    def col_copy(slots, send, recv, source, target):
        return pltpu.make_async_remote_copy(
            src_ref=slots.at[source],
            dst_ref=slots.at[source],
            send_sem=send.at[target],
            recv_sem=recv.at[source],
            device_id={"sp": target * RING + mx},
            device_id_type=MESH,
        )

    def send_row(slots, send, recv):
        for off in (2, 1, 3):
            row_copy(slots, send, recv, lax.rem(mx + off, RING)).start()

    def row_sum(slots, send, recv, order):
        all_of(slots.at[0 : RING - 1], send.at[0], recv.at[0]).wait_recv()
        acc = jnp.zeros((STATE, lanes), F32)
        log = jnp.zeros((1, lanes), F32)
        own, own_log = acc, log
        for at in order:
            own = jnp.where(mx == at, acc, own)
            own_log = jnp.where(mx == at, log, own_log)
            tail = slots[at, STATE : STATE + 1, :]
            acc = slots[at, 0:STATE, :] + jnp.exp(tail) * acc
            log = log + tail
        return own, own_log, acc, log

    message(grow, mx, grad, total)

    def project(i):
        x_copy(i).wait()
        rows = pl.ds(pl.multiple_of(i * xrows, xrows), xrows)
        p_s[rows, :] = nn(x_v[rows, :], w_v[...]).astype(BF16).astype(F32)

    def local(c):
        rows = block_rows(c)
        col = columns_of(c, (0, 1, 2, 3, 6, 7))
        pair = pl.ds(c * 2 * BLK, 2 * BLK)
        scores = tn(k_v[:, rows], q_v[:, rows])
        decay = jnp.concatenate(
            [
                jnp.exp(jnp.where(upper, stack_s[h * blocks + c : h * blocks + c + 1, :] - col[h], -1e30))
                for h in range(2)
            ],
            axis=0,
        )
        lm_s[pair, :] = decay
        te_s[rows, :] = jnp.where(first_head, col[4], col[5])
        se_s[rows, :] = jnp.where(first_head, col[2], col[3])
        dy_high, dy_low = halves(dy_s[rows, :])
        t_high, t_low = halves(jnp.concatenate([scores, scores], axis=0) * decay)
        tm_s[pair, :] = t_high
        u = folded(nn(t_high, jnp.concatenate([dy_high, dy_low], axis=1))) + nn(t_low, dy_high)
        u_s[rows, :] = jnp.where(first_head, u[0:BLK, :], u[BLK : 2 * BLK, :])

    def with_values(c):
        rows = block_rows(c)
        projected = p_s[rows, :]
        v = projected * sigmoid(projected)
        v_s[rows, :] = v
        bs_s[c] = folded(nn(k_v[:, rows], both(te_s[rows, :] * se_s[rows, :] * v)))

    x_copy(1).start()
    for c in range(blocks):
        if c == blocks // 4:
            pl.semaphore_wait(barrier, 2 * (RING - 1) + tp_count - 1)
            send_row(grow, gs_sem, gr_sem)
        if c == blocks // 2:
            for i in range(2, xchunks):
                x_copy(i).start()
        local(c)
    small[6].wait()

    def chunk(i, carry):
        project(i)
        return carry

    chunk(0, 0)
    own_grad, own_log, ring_grad, ring_log = row_sum(grow, gs_sem, gr_sem, (3, 2, 1, 0))
    message(gcol, mz, ring_grad, ring_log)
    for target in (1, 0, 2):

        @pl.when(target < mz)
        def _(target=target):
            col_copy(gcol, gs2_sem, gr2_sem, mz, target).start()

    lax.fori_loop(1, xchunks, chunk, 0)
    for_blocks(0, blocks, blocks, with_values)
    state = jnp.zeros((STATE, lanes), F32)
    for c in range(blocks):
        sst_s[c] = state
        state = fend_s[c : c + 1, :] * state + bs_s[c]
    last_s[...] = state
    message(srow, mx, state, total)
    send_row(srow, ss_sem, sr_sem)

    out_s[...] = jnp.zeros_like(out_s)
    for source in reversed(range(1, RING)):

        @pl.when(source > mz)
        def _(source=source):
            col_copy(gcol, gs2_sem, gr2_sem, source, mz).wait_recv()
            out_s[...] = gcol[source, 0:STATE, :] + jnp.exp(gcol[source, STATE : STATE + 1, :]) * out_s[...]

    out_s[...] = own_grad + jnp.exp(own_log) * out_s[...]
    after = jnp.zeros((1, lanes), F32)
    for c in reversed(range(blocks)):
        after = after + rend_s[c : c + 1, :]
        gst_s[c] = gst_s[c] + jnp.exp(after) * out_s[...]
    gst_s[blocks] = out_s[...]

    def value_gradient(c):
        rows = block_rows(c)
        u = u_s[rows, :] + te_s[rows, :] * folded(tn(k_v[:, rows], both(gst_s[c + 1])))
        u_s[rows, :] = u
        projected = p_s[rows, :]
        sig = sigmoid(projected)
        vg = se_s[rows, :] * u * sig * (1.0 + projected * (1.0 - sig))
        vgt_s[:, rows] = vg.astype(BF16).T

    for_blocks(0, blocks, blocks, value_gradient)

    def owner(dz, dx):
        return lax.rem(mz + dz, RING) * RING + lax.rem(mx + dx, RING)

    def on_axis(axis, dist):
        if axis == 0:
            return lax.rem(mz + dist, RING) * RING + mx
        return mz * RING + lax.rem(mx + dist, RING)

    def piece(half, dist, across):
        dz, dx = (dist, across) if half == 0 else (across, dist)
        return part.at[owner(dz, dx), half * HEAD : (half + 1) * HEAD, :]

    def far_copy(half, across):
        lane = half * RING + across
        return pltpu.make_async_remote_copy(
            src_ref=piece(half, 2, across),
            dst_ref=far_r.at[lane],
            send_sem=far_s.at[0],
            recv_sem=far_sem.at[lane],
            device_id={"sp": on_axis(half, 1 if across < 2 else 3)},
            device_id_type=MESH,
        )

    def near_copy(half, dist, across):
        lane = half * RING + across
        return pltpu.make_async_remote_copy(
            src_ref=piece(half, dist, across),
            dst_ref=near_r.at[2 * lane + (0 if dist == 1 else 1)],
            send_sem=near_s.at[0],
            recv_sem=near_sem.at[lane],
            device_id={"sp": on_axis(half, dist)},
            device_id_type=MESH,
        )

    def second_copy(half, across):
        return pltpu.make_async_remote_copy(
            src_ref=red_s.at[half * RING + across],
            dst_ref=second_r.at[half * (RING - 1) + across - 1],
            send_sem=second_s.at[0],
            recv_sem=second_sem.at[half],
            device_id={"sp": on_axis(1 - half, across)},
            device_id_type=MESH,
        )

    for group in ORDER:
        for dz, dx in group:
            dest = owner(dz, dx)
            columns = pl.ds(pl.multiple_of(dest * cols, cols), cols)
            part[dest] = nn(vgt_s[...], x_v[:, columns])
        for dz, dx in group:
            for half, dist, across in ((0, dz, dx), (1, dx, dz)):
                if dist == 2:
                    far_copy(half, across).start()
                elif (dist, across < 2) in ((1, False), (3, True)):
                    near_copy(half, dist, across).start()
    zero = jnp.zeros((BLK, lanes), BF16)
    lane_id = lax.broadcasted_iota(jnp.int32, (BLK, lanes), 1)
    yy_s[...] = jnp.zeros_like(yy_s)
    dd_s[...] = jnp.zeros_like(dd_s)

    def keep_head_sums(ref, c, a):
        first = jnp.sum(jnp.where(first_head, a, 0.0), axis=1, keepdims=True)
        second = jnp.sum(jnp.where(first_head, 0.0, a), axis=1, keepdims=True)
        ref[...] = jnp.where(lane_id == c, first, jnp.where(lane_id == blocks + c, second, ref[...]))

    def split_heads(a):
        return jnp.concatenate([jnp.where(first_head, a, zero), jnp.where(first_head, zero, a)], axis=0)

    def span_only(c):
        rows = block_rows(c)
        pair = pl.ds(pl.multiple_of(c * 2 * BLK, 2 * BLK), 2 * BLK)
        q, k = q_v[:, rows], k_v[:, rows]
        v = v_s[rows, :]
        sv = se_s[rows, :] * v
        sv_high, sv_low = halves(sv)
        by_head = split_heads(sv_high)
        m_s[rows, :] = folded(tn(tm_s[pair, :], jnp.concatenate([by_head, split_heads(sv_low)], axis=1)))
        d = nt(by_head, dy_s[rows, :].astype(BF16)) * lm_s[pair, :]
        d_high, d_low = halves(d[0:BLK, :] + d[BLK : 2 * BLK, :])
        kg_ref[:, rows] = nt(
            jnp.concatenate([q, q], axis=1), jnp.concatenate([d_high, d_low], axis=1)
        ) + nt(gst_s[c + 1].astype(BF16), (te_s[rows, :] * sv).astype(BF16))
        qg_ref[:, rows] = nn(jnp.concatenate([k, k], axis=1), jnp.concatenate([d_high, d_low], axis=0))
        keep_head_sums(dd_s, c, v * u_s[rows, :])

    def with_entering(c):
        rows = block_rows(c)
        dy, er = dy_s[rows, :], er_s[rows, :]
        mixed = m_s[rows, :] + er * folded(tn(q_v[:, rows], both(sst_s[c])))
        gate = gate_v[rows, :].astype(F32)
        sig = sigmoid(gate)
        gg_ref[rows, :] = cot_v[rows, :].astype(F32) * mixed * sig * (1.0 + gate * (1.0 - sig))
        qg_ref[:, rows] = qg_ref[:, rows] + nt(sst_s[c].astype(BF16), (er * dy).astype(BF16))
        keep_head_sums(yy_s, c, dy * mixed)

    steps = (4, blocks // 2, blocks * 3 // 4) if blocks >= 16 else (1, blocks // 2, blocks // 2)
    for_blocks(0, steps[1], steps[0], span_only)
    for dist, across in ((3, 2), (1, 0), (1, 1), (3, 3)):
        for half in range(2):
            far_copy(half, across).wait_recv()
            ref = piece(half, dist, across)
            ref[...] = ref[...] + far_r[half * RING + across]
            near_copy(half, dist, across).start()
    own_state, own_state_log, ring_state, ring_log = row_sum(srow, ss_sem, sr_sem, (0, 1, 2, 3))
    message(scol, mz, ring_state, ring_log)
    for target in range(1, RING):

        @pl.when(target > mz)
        def _(target=target):
            col_copy(scol, ss2_sem, sr2_sem, mz, target).start()

    for_blocks(steps[1], steps[2], steps[0], span_only)

    for across in (2, 1, 3, 0):
        if across == 1:
            for_blocks(steps[2], blocks, steps[0], span_only)
        for half in range(2):
            lane = half * RING + across
            all_of(near_r.at[2 * lane : 2 * lane + 2], near_s.at[0], near_sem.at[lane]).wait_recv()
            red_s[lane] = piece(half, 0, across)[...] + near_r[2 * lane] + near_r[2 * lane + 1]
            if across != 0:
                second_copy(half, across).start()

    inc_s[...] = jnp.zeros_like(inc_s)
    for source in range(RING - 1):

        @pl.when(source < mz)
        def _(source=source):
            col_copy(scol, ss2_sem, sr2_sem, source, mz).wait_recv()
            inc_s[...] = scol[source, 0:STATE, :] + jnp.exp(scol[source, STATE : STATE + 1, :]) * inc_s[...]

    inc_s[...] = own_state + jnp.exp(own_state_log) * inc_s[...]
    before = jnp.zeros((1, lanes), F32)
    for c in range(blocks):
        full = sst_s[c] + jnp.exp(before) * inc_s[...]
        sst_s[c] = full
        before = before + rend_s[c : c + 1, :]
        if c > 0:
            ee_s[c - 1 : c, :] = jnp.sum(full * gst_s[c], axis=0, keepdims=True)
    last = last_s[...] + jnp.exp(before) * inc_s[...]
    ee_s[blocks - 1 : blocks, :] = jnp.sum(last * gst_s[blocks], axis=0, keepdims=True)

    later = blocks * 3 // 4 if blocks >= 8 else blocks // 2
    for_blocks(0, later, min(4, later), with_entering)

    squares = jnp.zeros((1, cols), F32)
    for half in range(2):
        at = half * (RING - 1)
        all_of(second_r.at[at : at + RING - 1], second_s.at[0], second_sem.at[half]).wait_recv()
        done = red_s[half * RING] + second_r[at] + second_r[at + 1] + second_r[at + 2]
        red_s[half * RING] = done
        squares = squares + jnp.sum(done * done, axis=0, keepdims=True)

    def norm_copy(source, target):
        return pltpu.make_async_remote_copy(
            src_ref=nmsg,
            dst_ref=nslots.at[source],
            send_sem=norm_s.at[0],
            recv_sem=norm_r.at[0],
            device_id={"tp": target},
            device_id_type=MESH,
        )

    nmsg[...] = jnp.broadcast_to(squares, (8, cols))
    for off in range(1, tp_count):
        norm_copy(my_tp, lax.rem(my_tp + off, tp_count)).start()
    for_blocks(later, blocks, min(4, blocks - later), with_entering)
    ends = ee_s[...]
    end_cols = jnp.concatenate(
        [
            jnp.sum(ends[:, 0:HEAD], axis=1, keepdims=True),
            jnp.sum(ends[:, HEAD:lanes], axis=1, keepdims=True),
        ],
        axis=0,
    )
    direct = dd_s[...].T[0 : 2 * blocks, :]
    log_grad = nn(yy_s[...].T[0 : 2 * blocks, :] - step * direct, lower.astype(F32), HIGHEST) + end_cols
    decay_grad = (direct - rate * log_grad) * sigmoid(pre)
    for h in range(2):
        for c in range(blocks):
            dg_ref[h : h + 1, c * BLK : (c + 1) * BLK] = decay_grad[h * blocks + c : h * blocks + c + 1, :]
    for half in range(2):
        wg_ref[:, half * HEAD : (half + 1) * HEAD] = red_s[half * RING].T
    norms = squares
    if tp_count > 1:
        all_of(nslots.at[0 : tp_count - 1], norm_s.at[0], norm_r.at[0]).wait_recv()
    for off in range(1, tp_count):
        norms = norms + nslots[lax.rem(my_tp + off, tp_count), 0:1, :]
    rn_ref[...] = norms

    all_of(grow.at[0 : RING - 1], gs_sem.at[0], gr_sem.at[0]).wait_send()
    all_of(srow.at[0 : RING - 1], ss_sem.at[0], sr_sem.at[0]).wait_send()
    for target in range(RING):

        @pl.when(target < mz)
        def _(target=target):
            col_copy(gcol, gs2_sem, gr2_sem, mz, target).wait_send()

        @pl.when(target > mz)
        def _(target=target):
            col_copy(scol, ss2_sem, sr2_sem, mz, target).wait_send()

    all_of(far_r, far_s.at[0], far_sem.at[0]).wait_send()
    all_of(near_r, near_s.at[0], near_sem.at[0]).wait_send()
    all_of(second_r, second_s.at[0], second_sem.at[0]).wait_send()
    if tp_count > 1:
        all_of(nslots.at[0 : tp_count - 1], norm_s.at[0], norm_r.at[0]).wait_send()


def put_out(*refs):
    sources, targets, sems = refs[:6], refs[6:12], refs[12]
    copies = [pltpu.make_async_copy(s, t, sems.at[i]) for i, (s, t) in enumerate(zip(sources, targets))]
    for copy in copies:
        copy.start()
    for copy in copies:
        copy.wait()


def shards(sp_count, tp_count, block_input, value_weight, key_rows, query_rows, decay_pre, decay_log, gate_rows, out_grad):
    tokens, width = block_input.shape
    blocks = tokens // BLK
    lanes = 2 * HEAD
    cols = width // sp_count
    vmem = lambda shape, dtype=F32: pltpu.VMEM(shape, dtype)
    dma = lambda *shape: pltpu.SemaphoreType.DMA(shape)
    state_msg = (STATE + 8, lanes)
    scratch = [
        vmem((tokens, lanes)),
        vmem((tokens, width), BF16), vmem((width, lanes), BF16), vmem((STATE, tokens), BF16), vmem((STATE, tokens), BF16),
        vmem((2, tokens)), pltpu.SMEM((2,), F32), vmem((tokens, lanes), BF16), vmem((tokens, lanes), BF16),
        vmem((2 * blocks, BLK)), vmem((BLK, BLK)), vmem((blocks, lanes)), vmem((blocks, lanes)),
        vmem((tokens, lanes)), vmem((2 * tokens, BLK), BF16), vmem((2 * tokens, BLK)), vmem((tokens, lanes)),
        vmem((tokens, lanes)), vmem((tokens, lanes)), vmem((tokens, lanes)), vmem((tokens, lanes)), vmem((tokens, lanes)),
        vmem((blocks + 1, STATE, lanes)), vmem((blocks, STATE, lanes)), vmem((blocks, STATE, lanes)),
        vmem((STATE, lanes)), vmem((STATE, lanes)), vmem((lanes, tokens), BF16),
        vmem((BLK, lanes)), vmem((BLK, lanes)), vmem((blocks, lanes)),
        vmem((STATE, lanes)), *(vmem((RING, *state_msg)) for _ in range(4)),
        vmem((sp_count, lanes, cols)), vmem((8, HEAD, cols)), vmem((16, HEAD, cols)), vmem((8, HEAD, cols)),
        vmem((6, HEAD, cols)),
        vmem((8, cols)), vmem((tp_count, 8, cols)),
        dma(7), dma(max(2, tokens // (4 * BLK))), *(dma(1) for _ in range(4)), *(dma(RING) for _ in range(4)),
        dma(1), dma(8), dma(1), dma(8), dma(1), dma(2), dma(1), dma(1),
    ]
    hbm = pl.BlockSpec(memory_space=pltpu.HBM)
    in_vmem = pl.BlockSpec(memory_space=pltpu.VMEM)
    outs = pl.pallas_call(
        functools.partial(mixer, sp_count, tp_count),
        out_shape=(
            jax.ShapeDtypeStruct((STATE, tokens), F32),
            jax.ShapeDtypeStruct((STATE, tokens), F32),
            jax.ShapeDtypeStruct((2, tokens), F32),
            jax.ShapeDtypeStruct((tokens, lanes), F32),
            jax.ShapeDtypeStruct((cols, lanes), F32),
            jax.ShapeDtypeStruct((1, cols), F32),
        ),
        in_specs=[hbm] * 8,
        out_specs=tuple([in_vmem] * 6),
        scratch_shapes=scratch,
        compiler_params=pltpu.CompilerParams(
            collective_id=0, has_side_effects=True, vmem_limit_bytes=46 * 1024 * 1024
        ),
        name="mixer",
    )(
        *(pltpu.with_memory_space_constraint(a, pltpu.HBM) for a in (block_input, value_weight, key_rows.T, query_rows.T, decay_pre)),
        pltpu.with_memory_space_constraint(decay_log, pltpu.HBM),
        *(pltpu.with_memory_space_constraint(a, pltpu.HBM) for a in (gate_rows, out_grad)),
    )
    kg, qg, dg, gg, wg, rn = pl.pallas_call(
        put_out,
        out_shape=tuple(jax.ShapeDtypeStruct(o.shape, o.dtype) for o in outs),
        in_specs=[in_vmem] * 6,
        out_specs=tuple([hbm] * 6),
        scratch_shapes=[dma(6)],
        compiler_params=pltpu.CompilerParams(vmem_limit_bytes=8 * 1024 * 1024),
        name="put_out",
    )(*outs)
    return kg.T, qg.T, dg, gg, wg, rn.reshape(cols)


def solution(mesh):
    in_specs = (
        P("sp", None),
        P(None, "tp"),
        P("sp", "tp"),
        P("sp", "tp"),
        P("tp", "sp"),
        P("tp"),
        P("sp", "tp"),
        P("sp", "tp"),
    )
    out_specs = (P("sp", "tp"), P("sp", "tp"), P("tp", "sp"), P("sp", "tp"), P("sp", "tp"), P("sp"))
    body = functools.partial(shards, mesh.shape["sp"], mesh.shape["tp"])
    return jax.shard_map(body, mesh=mesh, in_specs=in_specs, out_specs=out_specs, check_vma=False)
```

```python
import functools

import jax
import jax.numpy as jnp
from jax import lax
from jax.experimental import pallas as pl
from jax.experimental.pallas import tpu as pltpu
from jax.sharding import PartitionSpec as P

HEAD = 64
STATE = 64
BLK = 128
RING = 4
F32 = jnp.float32
BF16 = jnp.bfloat16
HIGHEST = lax.Precision.HIGHEST
MESH = pl.DeviceIdType.MESH

ORDER = [
    [(2, 2)], [(2, 0), (0, 2)], [(2, 1), (1, 2)], [(2, 3), (3, 2)], [(1, 3), (3, 1)],
    [(3, 3), (1, 1)], [(1, 0), (0, 1)], [(3, 0), (0, 3)], [(0, 0)],
]


def nn(a, b, precision=None):
    return lax.dot_general(a, b, (((1,), (0,)), ((), ())), precision=precision, preferred_element_type=F32)


def nt(a, b, precision=None):
    return lax.dot_general(a, b, (((1,), (1,)), ((), ())), precision=precision, preferred_element_type=F32)


def tn(a, b, precision=None):
    return lax.dot_general(a, b, (((0,), (0,)), ((), ())), precision=precision, preferred_element_type=F32)


def halves(a):
    high = a.astype(BF16)
    return high, (a - high.astype(F32)).astype(BF16)


def both(a):
    return jnp.concatenate(halves(a), axis=1)


def folded(a):
    width = a.shape[1] // 2
    return a[:, :width] + a[:, width:]


def softplus(a):
    return jnp.maximum(a, 0.0) + jnp.log1p(jnp.exp(-jnp.abs(a)))


def sigmoid(a):
    return 1.0 / (1.0 + jnp.exp(-a))


def mixer(
    sp_count,
    tp_count,
    x_hbm, w_hbm, k_hbm, q_hbm, pre_hbm, rate_hbm, gate_hbm, cot_hbm,
    kg_ref, qg_ref, dg_ref, gg_ref, wg_ref, rn_ref,
    m_s,
    x_v, w_v, k_v, q_v, pre_v, rate_ref, gate_v, cot_v,
    rows_s, stack_s, rend_s, fend_s,
    dy_s, tm_s, lm_s, er_s, te_s, se_s, p_s, v_s, u_s,
    gst_s, sst_s, bs_s, out_s, inc_s, vgt_s,
    yy_s, dd_s, ee_s,
    last_s, grow, gcol, srow, scol,
    part, far_r, near_r, red_s, second_r,
    nmsg, nslots,
    in_sem, x_sem, gs_sem, gr_sem, ss_sem, sr_sem, gs2_sem, gr2_sem, ss2_sem, sr2_sem,
    far_s, far_sem, near_s, near_sem, second_s, second_sem, norm_s, norm_r,
):
    tokens, width = x_v.shape
    blocks = tokens // BLK
    lanes = 2 * HEAD
    cols = width // sp_count
    me = lax.axis_index("sp")
    my_tp = lax.axis_index("tp")
    mz, mx = lax.div(me, RING), lax.rem(me, RING)

    barrier = pltpu.get_barrier_semaphore()
    for off in range(1, RING):
        for peer in (mz * RING + lax.rem(mx + off, RING), lax.rem(mz + off, RING) * RING + mx):
            pl.semaphore_signal(barrier, inc=1, device_id={"sp": peer}, device_id_type=MESH)
    for off in range(1, tp_count):
        pl.semaphore_signal(
            barrier, inc=1, device_id={"tp": lax.rem(my_tp + off, tp_count)}, device_id_type=MESH
        )

    small = [
        pltpu.make_async_copy(src, dst, in_sem.at[i])
        for i, (src, dst) in enumerate(
            [
                (pre_hbm, pre_v), (rate_hbm, rate_ref), (gate_hbm, gate_v), (cot_hbm, cot_v), (q_hbm, q_v), (k_hbm, k_v), (w_hbm, w_v)
            ]
        )
    ]
    for copy in small[:6]:
        copy.start()
    xrows = tokens // x_sem.shape[0]
    xchunks = tokens // xrows

    def x_copy(i):
        rows = pl.ds(pl.multiple_of(i * xrows, xrows), xrows)
        return pltpu.make_async_copy(x_hbm.at[rows], x_v.at[rows], x_sem.at[i])

    small[0].wait()
    small[1].wait()
    for h in range(2):
        for c in range(blocks):
            rows_s[h * blocks + c : h * blocks + c + 1, :] = pre_v[h : h + 1, c * BLK : (c + 1) * BLK]
    pre = rows_s[...]
    row_id = lax.broadcasted_iota(jnp.int32, (2 * blocks, BLK), 0)
    rate = jnp.where(
        row_id < blocks,
        jnp.exp(jnp.full((2 * blocks, BLK), rate_ref[0], F32)),
        jnp.exp(jnp.full((2 * blocks, BLK), rate_ref[1], F32)),
    )
    step = softplus(pre)
    sq_row = lax.broadcasted_iota(jnp.int32, (BLK, BLK), 0)
    sq_col = lax.broadcasted_iota(jnp.int32, (BLK, BLK), 1)
    upper = sq_row <= sq_col
    lower = sq_row >= sq_col
    run = nn(-rate * step, (sq_row <= sq_col).astype(F32), HIGHEST)
    if 8 * blocks < BLK:
        stack_s[...] = jnp.zeros_like(stack_s)
    stack_s[0 : 2 * blocks, :] = run
    stack_s[2 * blocks : 4 * blocks, :] = step
    stack_s[4 * blocks : 6 * blocks, :] = jnp.exp(run)
    stack_s[6 * blocks : 8 * blocks, :] = jnp.exp(run[:, BLK - 1 : BLK] - run)
    turned = stack_s[...].T
    rend = jnp.where(
        lax.broadcasted_iota(jnp.int32, (blocks, lanes), 1) < HEAD,
        run[0:blocks, BLK - 1 : BLK],
        run[blocks : 2 * blocks, BLK - 1 : BLK],
    )
    rend_s[...] = rend
    fend_s[...] = jnp.exp(rend)
    first_head = lax.broadcasted_iota(jnp.int32, (BLK, lanes), 1) < HEAD
    for copy in small[2:6]:
        copy.wait()
    small[6].start()
    x_copy(0).start()

    def block_rows(c):
        return pl.ds(c * BLK if isinstance(c, int) else pl.multiple_of(c * BLK, BLK), BLK)

    def for_blocks(start, stop, unroll, body):
        if unroll == stop - start:
            for c in range(start, stop):
                body(c)
            return

        def step_of(i, carry):
            for b in range(unroll):
                body(start + i * unroll + b)
            return carry

        lax.fori_loop(0, (stop - start) // unroll, step_of, 0)

    def columns_of(c, kinds):
        return [jnp.broadcast_to(turned[:, i * blocks + c : i * blocks + c + 1], (BLK, BLK)) for i in kinds]

    def prepare(c):
        rows = block_rows(c)
        er = jnp.where(first_head, *columns_of(c, (4, 5)))
        er_s[rows, :] = er
        gate = gate_v[rows, :].astype(F32)
        dy = cot_v[rows, :].astype(F32) * gate * sigmoid(gate)
        dy_s[rows, :] = dy
        bs_s[c] = folded(nn(q_v[:, rows], both(er * dy)))

    for_blocks(0, blocks, blocks, prepare)
    grad = jnp.zeros((STATE, lanes), F32)
    total = jnp.zeros((1, lanes), F32)
    for c in reversed(range(blocks)):
        end = rend_s[c : c + 1, :]
        grad = fend_s[c : c + 1, :] * grad + bs_s[c]
        total = total + end
        gst_s[c] = grad
    def message(ref, at, value, log):
        ref[at, 0:STATE, :] = value
        ref[at, STATE : STATE + 8, :] = jnp.broadcast_to(log, (8, lanes))

    def row_copy(slots, send, recv, target):
        return pltpu.make_async_remote_copy(
            src_ref=slots.at[mx],
            dst_ref=slots.at[mx],
            send_sem=send.at[0],
            recv_sem=recv.at[0],
            device_id={"sp": mz * RING + target},
            device_id_type=MESH,
        )

    def all_of(refs, send, recv):
        return pltpu.make_async_remote_copy(
            src_ref=refs,
            dst_ref=refs,
            send_sem=send,
            recv_sem=recv,
            device_id={"sp": mz * RING + lax.rem(mx + 1, RING)},
            device_id_type=MESH,
        )

    def col_copy(slots, send, recv, source, target):
        return pltpu.make_async_remote_copy(
            src_ref=slots.at[source],
            dst_ref=slots.at[source],
            send_sem=send.at[target],
            recv_sem=recv.at[source],
            device_id={"sp": target * RING + mx},
            device_id_type=MESH,
        )

    def send_row(slots, send, recv):
        for off in (2, 1, 3):
            row_copy(slots, send, recv, lax.rem(mx + off, RING)).start()

    def row_sum(slots, send, recv, order):
        all_of(slots.at[0 : RING - 1], send.at[0], recv.at[0]).wait_recv()
        acc = jnp.zeros((STATE, lanes), F32)
        log = jnp.zeros((1, lanes), F32)
        own, own_log = acc, log
        for at in order:
            own = jnp.where(mx == at, acc, own)
            own_log = jnp.where(mx == at, log, own_log)
            tail = slots[at, STATE : STATE + 1, :]
            acc = slots[at, 0:STATE, :] + jnp.exp(tail) * acc
            log = log + tail
        return own, own_log, acc, log

    message(grow, mx, grad, total)

    def project(i):
        x_copy(i).wait()
        rows = pl.ds(pl.multiple_of(i * xrows, xrows), xrows)
        p_s[rows, :] = nn(x_v[rows, :], w_v[...]).astype(BF16).astype(F32)

    zero = jnp.zeros((BLK, lanes), BF16)

    def local(c):
        rows = block_rows(c)
        col = columns_of(c, (0, 1, 2, 3, 6, 7))
        pair = pl.ds(c * 2 * BLK, 2 * BLK)
        scores = tn(k_v[:, rows], q_v[:, rows])
        decay = jnp.concatenate(
            [
                jnp.exp(jnp.where(upper, stack_s[h * blocks + c : h * blocks + c + 1, :] - col[h], -1e30))
                for h in range(2)
            ],
            axis=0,
        )
        lm_s[pair, :] = decay
        te_s[rows, :] = jnp.where(first_head, col[4], col[5])
        se_s[rows, :] = jnp.where(first_head, col[2], col[3])
        dy_high, dy_low = halves(dy_s[rows, :])
        t_high, t_low = halves(jnp.concatenate([scores, scores], axis=0) * decay)
        tm_s[pair, :] = t_high
        u = folded(
            nn(
                jnp.concatenate([t_high, t_low], axis=1),
                jnp.concatenate(
                    [jnp.concatenate([dy_high, dy_low], axis=1), jnp.concatenate([dy_high, zero], axis=1)], axis=0
                ),
            )
        )
        u_s[rows, :] = jnp.where(first_head, u[0:BLK, :], u[BLK : 2 * BLK, :])

    def with_values(c):
        rows = block_rows(c)
        projected = p_s[rows, :]
        v = projected * sigmoid(projected)
        v_s[rows, :] = v
        bs_s[c] = folded(nn(k_v[:, rows], both(te_s[rows, :] * se_s[rows, :] * v)))

    x_copy(1).start()
    for c in range(blocks):
        if c == 0:
            pl.semaphore_wait(barrier, 2 * (RING - 1) + tp_count - 1)
            send_row(grow, gs_sem, gr_sem)
        if c == blocks // 2:
            for i in range(2, xchunks):
                x_copy(i).start()
        local(c)
    small[6].wait()

    def chunk(i, carry):
        project(i)
        return carry

    chunk(0, 0)
    own_grad, own_log, ring_grad, ring_log = row_sum(grow, gs_sem, gr_sem, (3, 2, 1, 0))
    message(gcol, mz, ring_grad, ring_log)
    for target in (1, 0, 2):

        @pl.when(target < mz)
        def _(target=target):
            col_copy(gcol, gs2_sem, gr2_sem, mz, target).start()

    lax.fori_loop(1, xchunks, chunk, 0)
    for_blocks(0, blocks, blocks, with_values)
    state = jnp.zeros((STATE, lanes), F32)
    for c in range(blocks):
        sst_s[c] = state
        state = fend_s[c : c + 1, :] * state + bs_s[c]
    last_s[...] = state
    message(srow, mx, state, total)
    send_row(srow, ss_sem, sr_sem)

    out_s[...] = jnp.zeros_like(out_s)
    for source in reversed(range(1, RING)):

        @pl.when(source > mz)
        def _(source=source):
            col_copy(gcol, gs2_sem, gr2_sem, source, mz).wait_recv()
            out_s[...] = gcol[source, 0:STATE, :] + jnp.exp(gcol[source, STATE : STATE + 1, :]) * out_s[...]

    out_s[...] = own_grad + jnp.exp(own_log) * out_s[...]
    after = jnp.zeros((1, lanes), F32)
    for c in reversed(range(blocks)):
        after = after + rend_s[c : c + 1, :]
        gst_s[c] = gst_s[c] + jnp.exp(after) * out_s[...]
    gst_s[blocks] = out_s[...]

    def value_gradient(c):
        rows = block_rows(c)
        u = u_s[rows, :] + te_s[rows, :] * folded(tn(k_v[:, rows], both(gst_s[c + 1])))
        u_s[rows, :] = u
        projected = p_s[rows, :]
        sig = sigmoid(projected)
        vg = se_s[rows, :] * u * sig * (1.0 + projected * (1.0 - sig))
        vgt_s[:, rows] = vg.astype(BF16).T

    for_blocks(0, blocks, blocks, value_gradient)

    def owner(dz, dx):
        return lax.rem(mz + dz, RING) * RING + lax.rem(mx + dx, RING)

    def on_axis(axis, dist):
        if axis == 0:
            return lax.rem(mz + dist, RING) * RING + mx
        return mz * RING + lax.rem(mx + dist, RING)

    def piece(half, dist, across):
        dz, dx = (dist, across) if half == 0 else (across, dist)
        return part.at[owner(dz, dx), half * HEAD : (half + 1) * HEAD, :]

    def far_copy(half, across):
        lane = half * RING + across
        return pltpu.make_async_remote_copy(
            src_ref=piece(half, 2, across),
            dst_ref=far_r.at[lane],
            send_sem=far_s.at[0],
            recv_sem=far_sem.at[lane],
            device_id={"sp": on_axis(half, 1 if across < 2 else 3)},
            device_id_type=MESH,
        )

    def near_copy(half, dist, across):
        lane = half * RING + across
        return pltpu.make_async_remote_copy(
            src_ref=piece(half, dist, across),
            dst_ref=near_r.at[2 * lane + (0 if dist == 1 else 1)],
            send_sem=near_s.at[0],
            recv_sem=near_sem.at[lane],
            device_id={"sp": on_axis(half, dist)},
            device_id_type=MESH,
        )

    def second_copy(half, across):
        return pltpu.make_async_remote_copy(
            src_ref=red_s.at[half * RING + across],
            dst_ref=second_r.at[half * (RING - 1) + across - 1],
            send_sem=second_s.at[0],
            recv_sem=second_sem.at[half],
            device_id={"sp": on_axis(1 - half, across)},
            device_id_type=MESH,
        )

    for group in ORDER:
        for dz, dx in group:
            dest = owner(dz, dx)
            columns = pl.ds(pl.multiple_of(dest * cols, cols), cols)
            part[dest] = nn(vgt_s[...], x_v[:, columns])
        for dz, dx in group:
            for half, dist, across in ((0, dz, dx), (1, dx, dz)):
                if dist == 2:
                    far_copy(half, across).start()
                elif (dist, across < 2) in ((1, False), (3, True)):
                    near_copy(half, dist, across).start()
    lane_id = lax.broadcasted_iota(jnp.int32, (BLK, lanes), 1)
    yy_s[...] = jnp.zeros_like(yy_s)
    dd_s[...] = jnp.zeros_like(dd_s)

    def keep_head_sums(ref, c, a):
        first = jnp.sum(jnp.where(first_head, a, 0.0), axis=1, keepdims=True)
        second = jnp.sum(jnp.where(first_head, 0.0, a), axis=1, keepdims=True)
        ref[...] = jnp.where(lane_id == c, first, jnp.where(lane_id == blocks + c, second, ref[...]))

    def split_heads(a):
        return jnp.concatenate([jnp.where(first_head, a, zero), jnp.where(first_head, zero, a)], axis=0)

    def span_only(c):
        rows = block_rows(c)
        pair = pl.ds(pl.multiple_of(c * 2 * BLK, 2 * BLK), 2 * BLK)
        q, k = q_v[:, rows], k_v[:, rows]
        v = v_s[rows, :]
        sv = se_s[rows, :] * v
        sv_high, sv_low = halves(sv)
        by_head = split_heads(sv_high)
        m_s[rows, :] = folded(tn(tm_s[pair, :], jnp.concatenate([by_head, split_heads(sv_low)], axis=1)))
        d = nt(by_head, dy_s[rows, :].astype(BF16)) * lm_s[pair, :]
        d_high, d_low = halves(d[0:BLK, :] + d[BLK : 2 * BLK, :])
        kg_ref[:, rows] = nt(
            jnp.concatenate([q, q], axis=1), jnp.concatenate([d_high, d_low], axis=1)
        ) + nt(gst_s[c + 1].astype(BF16), (te_s[rows, :] * sv).astype(BF16))
        qg_ref[:, rows] = nn(jnp.concatenate([k, k], axis=1), jnp.concatenate([d_high, d_low], axis=0))
        keep_head_sums(dd_s, c, v * u_s[rows, :])

    def with_entering(c):
        rows = block_rows(c)
        dy, er = dy_s[rows, :], er_s[rows, :]
        mixed = m_s[rows, :] + er * folded(tn(q_v[:, rows], both(sst_s[c])))
        gate = gate_v[rows, :].astype(F32)
        sig = sigmoid(gate)
        gg_ref[rows, :] = cot_v[rows, :].astype(F32) * mixed * sig * (1.0 + gate * (1.0 - sig))
        qg_ref[:, rows] = qg_ref[:, rows] + nt(sst_s[c].astype(BF16), (er * dy).astype(BF16))
        keep_head_sums(yy_s, c, dy * mixed)

    steps = (4, blocks // 2, blocks * 3 // 4) if blocks >= 16 else (1, blocks // 2, blocks // 2)
    for_blocks(0, steps[1], steps[0], span_only)
    for dist, across in ((3, 2), (1, 0), (1, 1), (3, 3)):
        for half in range(2):
            far_copy(half, across).wait_recv()
            ref = piece(half, dist, across)
            ref[...] = ref[...] + far_r[half * RING + across]
            near_copy(half, dist, across).start()
    own_state, own_state_log, ring_state, ring_log = row_sum(srow, ss_sem, sr_sem, (0, 1, 2, 3))
    message(scol, mz, ring_state, ring_log)
    for target in range(1, RING):

        @pl.when(target > mz)
        def _(target=target):
            col_copy(scol, ss2_sem, sr2_sem, mz, target).start()

    for_blocks(steps[1], steps[2], steps[0], span_only)

    for across in (2, 1, 3, 0):
        if across == 1:
            for_blocks(steps[2], blocks, steps[0], span_only)
        for half in range(2):
            lane = half * RING + across
            all_of(near_r.at[2 * lane : 2 * lane + 2], near_s.at[0], near_sem.at[lane]).wait_recv()
            red_s[lane] = piece(half, 0, across)[...] + near_r[2 * lane] + near_r[2 * lane + 1]
            if across != 0:
                second_copy(half, across).start()

    inc_s[...] = jnp.zeros_like(inc_s)
    for source in range(RING - 1):

        @pl.when(source < mz)
        def _(source=source):
            col_copy(scol, ss2_sem, sr2_sem, source, mz).wait_recv()
            inc_s[...] = scol[source, 0:STATE, :] + jnp.exp(scol[source, STATE : STATE + 1, :]) * inc_s[...]

    inc_s[...] = own_state + jnp.exp(own_state_log) * inc_s[...]
    before = jnp.zeros((1, lanes), F32)
    for c in range(blocks):
        full = sst_s[c] + jnp.exp(before) * inc_s[...]
        sst_s[c] = full
        before = before + rend_s[c : c + 1, :]
        if c > 0:
            ee_s[c - 1 : c, :] = jnp.sum(full * gst_s[c], axis=0, keepdims=True)
    last = last_s[...] + jnp.exp(before) * inc_s[...]
    ee_s[blocks - 1 : blocks, :] = jnp.sum(last * gst_s[blocks], axis=0, keepdims=True)

    later = blocks * 3 // 4 if blocks >= 8 else blocks // 2
    for_blocks(0, later, min(4, later), with_entering)

    squares = jnp.zeros((1, cols), F32)
    for half in range(2):
        at = half * (RING - 1)
        all_of(second_r.at[at : at + RING - 1], second_s.at[0], second_sem.at[half]).wait_recv()
        done = red_s[half * RING] + second_r[at] + second_r[at + 1] + second_r[at + 2]
        red_s[half * RING] = done
        squares = squares + jnp.sum(done * done, axis=0, keepdims=True)

    def norm_copy(source, target):
        return pltpu.make_async_remote_copy(
            src_ref=nmsg,
            dst_ref=nslots.at[source],
            send_sem=norm_s.at[0],
            recv_sem=norm_r.at[0],
            device_id={"tp": target},
            device_id_type=MESH,
        )

    nmsg[...] = jnp.broadcast_to(squares, (8, cols))
    for off in range(1, tp_count):
        norm_copy(my_tp, lax.rem(my_tp + off, tp_count)).start()
    for_blocks(later, blocks, min(4, blocks - later), with_entering)
    ends = ee_s[...]
    end_cols = jnp.concatenate(
        [
            jnp.sum(ends[:, 0:HEAD], axis=1, keepdims=True),
            jnp.sum(ends[:, HEAD:lanes], axis=1, keepdims=True),
        ],
        axis=0,
    )
    direct = dd_s[...].T[0 : 2 * blocks, :]
    log_grad = nn(yy_s[...].T[0 : 2 * blocks, :] - step * direct, lower.astype(F32), HIGHEST) + end_cols
    decay_grad = (direct - rate * log_grad) * sigmoid(pre)
    for h in range(2):
        for c in range(blocks):
            dg_ref[h : h + 1, c * BLK : (c + 1) * BLK] = decay_grad[h * blocks + c : h * blocks + c + 1, :]
    for half in range(2):
        wg_ref[:, half * HEAD : (half + 1) * HEAD] = red_s[half * RING].T
    norms = squares
    if tp_count > 1:
        all_of(nslots.at[0 : tp_count - 1], norm_s.at[0], norm_r.at[0]).wait_recv()
    for off in range(1, tp_count):
        norms = norms + nslots[lax.rem(my_tp + off, tp_count), 0:1, :]
    rn_ref[...] = norms

    all_of(grow.at[0 : RING - 1], gs_sem.at[0], gr_sem.at[0]).wait_send()
    all_of(srow.at[0 : RING - 1], ss_sem.at[0], sr_sem.at[0]).wait_send()
    for target in range(RING):

        @pl.when(target < mz)
        def _(target=target):
            col_copy(gcol, gs2_sem, gr2_sem, mz, target).wait_send()

        @pl.when(target > mz)
        def _(target=target):
            col_copy(scol, ss2_sem, sr2_sem, mz, target).wait_send()

    all_of(far_r, far_s.at[0], far_sem.at[0]).wait_send()
    all_of(near_r, near_s.at[0], near_sem.at[0]).wait_send()
    all_of(second_r, second_s.at[0], second_sem.at[0]).wait_send()
    if tp_count > 1:
        all_of(nslots.at[0 : tp_count - 1], norm_s.at[0], norm_r.at[0]).wait_send()


def put_out(*refs):
    sources, targets, sems = refs[:6], refs[6:12], refs[12]
    copies = [pltpu.make_async_copy(s, t, sems.at[i]) for i, (s, t) in enumerate(zip(sources, targets))]
    for copy in copies:
        copy.start()
    for copy in copies:
        copy.wait()


def shards(sp_count, tp_count, block_input, value_weight, key_rows, query_rows, decay_pre, decay_log, gate_rows, out_grad):
    tokens, width = block_input.shape
    blocks = tokens // BLK
    lanes = 2 * HEAD
    cols = width // sp_count
    vmem = lambda shape, dtype=F32: pltpu.VMEM(shape, dtype)
    dma = lambda *shape: pltpu.SemaphoreType.DMA(shape)
    state_msg = (STATE + 8, lanes)
    scratch = [
        vmem((tokens, lanes)),
        vmem((tokens, width), BF16), vmem((width, lanes), BF16), vmem((STATE, tokens), BF16), vmem((STATE, tokens), BF16),
        vmem((2, tokens)), pltpu.SMEM((2,), F32), vmem((tokens, lanes), BF16), vmem((tokens, lanes), BF16),
        vmem((2 * blocks, BLK)), vmem((BLK, BLK)), vmem((blocks, lanes)), vmem((blocks, lanes)),
        vmem((tokens, lanes)), vmem((2 * tokens, BLK), BF16), vmem((2 * tokens, BLK)), vmem((tokens, lanes)),
        vmem((tokens, lanes)), vmem((tokens, lanes)), vmem((tokens, lanes)), vmem((tokens, lanes)), vmem((tokens, lanes)),
        vmem((blocks + 1, STATE, lanes)), vmem((blocks, STATE, lanes)), vmem((blocks, STATE, lanes)),
        vmem((STATE, lanes)), vmem((STATE, lanes)), vmem((lanes, tokens), BF16),
        vmem((BLK, lanes)), vmem((BLK, lanes)), vmem((blocks, lanes)),
        vmem((STATE, lanes)), *(vmem((RING, *state_msg)) for _ in range(4)),
        vmem((sp_count, lanes, cols)), vmem((8, HEAD, cols)), vmem((16, HEAD, cols)), vmem((8, HEAD, cols)),
        vmem((6, HEAD, cols)),
        vmem((8, cols)), vmem((tp_count, 8, cols)),
        dma(7), dma(max(2, tokens // (4 * BLK))), *(dma(1) for _ in range(4)), *(dma(RING) for _ in range(4)),
        dma(1), dma(8), dma(1), dma(8), dma(1), dma(2), dma(1), dma(1),
    ]
    hbm = pl.BlockSpec(memory_space=pltpu.HBM)
    in_vmem = pl.BlockSpec(memory_space=pltpu.VMEM)
    outs = pl.pallas_call(
        functools.partial(mixer, sp_count, tp_count),
        out_shape=(
            jax.ShapeDtypeStruct((STATE, tokens), F32),
            jax.ShapeDtypeStruct((STATE, tokens), F32),
            jax.ShapeDtypeStruct((2, tokens), F32),
            jax.ShapeDtypeStruct((tokens, lanes), F32),
            jax.ShapeDtypeStruct((cols, lanes), F32),
            jax.ShapeDtypeStruct((1, cols), F32),
        ),
        in_specs=[hbm] * 8,
        out_specs=tuple([in_vmem] * 6),
        scratch_shapes=scratch,
        compiler_params=pltpu.CompilerParams(
            collective_id=0, has_side_effects=True, vmem_limit_bytes=46 * 1024 * 1024
        ),
        name="mixer",
    )(
        *(pltpu.with_memory_space_constraint(a, pltpu.HBM) for a in (block_input, value_weight, key_rows.T, query_rows.T, decay_pre)),
        pltpu.with_memory_space_constraint(decay_log, pltpu.HBM),
        *(pltpu.with_memory_space_constraint(a, pltpu.HBM) for a in (gate_rows, out_grad)),
    )
    kg, qg, dg, gg, wg, rn = pl.pallas_call(
        put_out,
        out_shape=tuple(jax.ShapeDtypeStruct(o.shape, o.dtype) for o in outs),
        in_specs=[in_vmem] * 6,
        out_specs=tuple([hbm] * 6),
        scratch_shapes=[dma(6)],
        compiler_params=pltpu.CompilerParams(vmem_limit_bytes=8 * 1024 * 1024),
        name="put_out",
    )(*outs)
    return kg.T, qg.T, dg, gg, wg, rn.reshape(cols)


def solution(mesh):
    in_specs = (
        P("sp", None),
        P(None, "tp"),
        P("sp", "tp"),
        P("sp", "tp"),
        P("tp", "sp"),
        P("tp"),
        P("sp", "tp"),
        P("sp", "tp"),
    )
    out_specs = (P("sp", "tp"), P("sp", "tp"), P("tp", "sp"), P("sp", "tp"), P("sp", "tp"), P("sp"))
    body = functools.partial(shards, mesh.shape["sp"], mesh.shape["tp"])
    return jax.shard_map(body, mesh=mesh, in_specs=in_specs, out_specs=out_specs, check_vma=False)
```
